128 devices in a mesh: sp: 32 (over z, y, core), tp: 4 (over x).
Axes of the slice: x: 4, y: 4, z: 4, core: 2. Of those that a mesh axis runs over, the one named last changes fastest.
Arguments:
- queries: bfloat16 [32768, 1024], P('sp', 'tp'), may hold values from -8 to 8
- keys: bfloat16 [32768, 256], P('sp', 'tp'), may hold values from -8 to 8
- values: bfloat16 [32768, 256], P('sp', 'tp'), may hold values from -18 to 18
- doc_ids: int32 [32768], P('sp'), may hold values from 0 to 7, never falling along the last dimension, each value on 1 to 16384 neighbouring positions
- sinks: float32 [16], P('tp'), may hold values from 0 to 4
- residual: bfloat16 [32768, 2048], P(('sp', 'tp')), may hold values from -12 to 12
- out_weight: bfloat16 [1024, 2048], P('tp'), may hold values from -0.1875 to 0.1875
- norm_gain: float32 [2048], replicated, may hold values from 0.1 to 1.9
- w_gate: bfloat16 [2048, 5632], P('sp', 'tp'), may hold values from -0.125 to 0.125
- w_value: bfloat16 [2048, 5632], P('sp', 'tp'), may hold values from -0.125 to 0.125
- conv_gate: float32 [3, 5632], P(None, 'tp'), may hold values from -3.5 to 3.5
- conv_value: float32 [3, 5632], P(None, 'tp'), may hold values from -3.5 to 3.5
- w_down: bfloat16 [5632, 2048], P('tp', 'sp'), may hold values from -0.078125 to 0.078125
Outputs:
- layer_out: bfloat16 [32768, 2048], P(('sp', 'tp'))
The draws below stay inside these ranges and needn't reach their ends.
All inputs are finite; a program needn't handle non-finite values.
Results may differ from the reference program's by a relative error of at most 0.012.
Values may be sent and summed in bfloat16 or wider, within the bound.
A program may use at most 128 MiB of HBM per device.

```python
import math
import jax
import jax.numpy as jnp
import numpy as np
from jax import lax

D = 2048
HEAD_DIM = 64
A_HEADS = 16
FF = 5632
WINDOW = 128
TOK_SP = 1024
TOKENS = 32768
A_Q = 1024
KV_W = 256
DOCS = 8
N_SP = 32


def draw_keys(key, part):
    base = jnp.clip(jax.random.normal(jax.random.fold_in(key, 1), (TOKENS, KV_W), jnp.float32), -8.0, 8.0)
    return base.astype(jnp.bfloat16)


def draw_queries(key, part):
    base = jnp.clip(jax.random.normal(jax.random.fold_in(key, 2), (TOKENS, A_Q), jnp.float32), -8.0, 8.0)
    return base.astype(jnp.bfloat16)


def draw_residual(key, part):
    base = jax.random.normal(jax.random.fold_in(key, 3), (TOKENS, D), jnp.float32)
    spread = jax.random.uniform(jax.random.fold_in(key, 4), (TOKENS, 1), jnp.float32, math.log(1.0 / 3.0), math.log(3.0))
    base = base * jnp.exp(spread)
    return jnp.clip(base, -12.0, 12.0).astype(jnp.bfloat16)


def shard_levels(key, shape, shards, least, top_value):
    gain, own = 1.0, jax.random.fold_in(key, 6)
    for dim, shards_of in shards:
        heights = jnp.exp(jax.random.uniform(jax.random.fold_in(own, dim), (shards_of,), jnp.float32, least / len(shards), top_value / len(shards)))
        gain = gain * jnp.repeat(heights, shape[dim] // shards_of).reshape([-1 if axis == dim else 1 for axis in range(len(shape))])
    return gain


def split_up(number_of, total, most, slope):
    portions = [(1 << 20) // math.isqrt(grade ** slope) + 1 for grade in range(2, number_of + 1)]
    rest, counts = total - most - (number_of - 1), [1] * (number_of - 1)
    while rest > 0:
        movable = [i for i in range(number_of - 1) if counts[i] < most]
        whole, left = sum([portions[i] for i in movable]), rest
        for i in movable:
            addition = min(most - counts[i], max(1, left * portions[i] // whole), rest)
            counts[i] = counts[i] + addition
            rest = rest - addition
    return np.array([most] + counts)


def ragged(stream_key, count, total, reach, slope):
    if count == 2:
        one = jax.random.randint(stream_key, (), max(1, total - reach), min(reach, total - 1) + 1)
        return jnp.stack([one, total - one])
    tallies = jnp.asarray(split_up(count, total, reach, slope), jnp.int32)
    couples = (count - 1) // 2
    donor, receiver = tallies[1:1 + 2 * couples:2], tallies[2:2 + 2 * couples:2]
    slack = jnp.minimum(donor - 1, reach - receiver)
    shifted = jax.random.randint(jax.random.fold_in(stream_key, 1), (couples,), 0, 1 << 20) % (slack + 1)
    tallies = tallies.at[1:1 + 2 * couples:2].set(donor - shifted).at[2:2 + 2 * couples:2].set(receiver + shifted)
    return tallies[jax.random.permutation(jax.random.fold_in(stream_key, 2), count)]


def bell_draw(stream_key, shape, deviation, limit, cuts=(), held_as=jnp.bfloat16):
    entries = deviation * jax.random.normal(stream_key, shape, jnp.float32)
    if cuts:
        entries = entries * shard_levels(stream_key, shape, cuts, -0.22, 0.18)
    return jnp.clip(entries, -limit, limit).astype(held_as)


def setup_inputs(seed: int = 0) -> dict:
    streams_of = jax.random.split(jax.random.key(seed), 14)
    queries = draw_queries(jax.random.fold_in(streams_of[13], 71), 0)
    keys = draw_keys(jax.random.fold_in(streams_of[13], 71), 0)
    values = bell_draw(streams_of[2], (TOKENS, KV_W), 3.0, 18.0, ((0, 32), (1, 4)))
    doc_ids = jnp.searchsorted(jnp.cumsum(ragged(streams_of[3], DOCS, TOKENS, TOKENS // 2, 0)), jnp.arange(TOKENS), side="right").astype(jnp.int32)
    sinks = jnp.clip(4.0 * jax.random.uniform(streams_of[4], (A_HEADS,), jnp.float32) ** shard_levels(streams_of[4], (A_HEADS,), ((0, 4),), -0.2, 0.2), 0.0, 4.0)
    residual = draw_residual(jax.random.fold_in(streams_of[13], 71), 0)
    out_weight = bell_draw(streams_of[6], (A_Q, D), A_Q ** -0.5, 0.1875, ((0, 4),))
    norm_gain = jnp.clip(1.0 + 0.18 * jax.random.normal(streams_of[7], (D,), jnp.float32), 0.1, 1.9)
    w_gate = bell_draw(streams_of[8], (D, FF), D ** -0.5, 0.125, ((0, 32), (1, 4)))
    w_value = bell_draw(streams_of[9], (D, FF), D ** -0.5, 0.125, ((0, 32), (1, 4)))
    conv_gate = bell_draw(streams_of[10], (3, FF), 3 ** -0.5, 3.5, ((1, 4),), jnp.float32)
    conv_value = bell_draw(streams_of[11], (3, FF), 3 ** -0.5, 3.5, ((1, 4),), jnp.float32)
    w_down = bell_draw(streams_of[12], (FF, D), FF ** -0.5, 0.078125, ((0, 4), (1, 32)))
    return dict(queries=queries, keys=keys, values=values, doc_ids=doc_ids, sinks=sinks, residual=residual, out_weight=out_weight, norm_gain=norm_gain, w_gate=w_gate, w_value=w_value, conv_gate=conv_gate, conv_value=conv_value, w_down=w_down)


def attend(query_rows, key_ext, value_ext, doc_rows, doc_ext, sinks):
    row_count = query_rows.shape[0]
    block_count = row_count // WINDOW
    kv_heads = key_ext.shape[1] // HEAD_DIM
    group_size = query_rows.shape[1] // (kv_heads * HEAD_DIM)

    def band(t):
        lower = t[:row_count].reshape((block_count, WINDOW) + t.shape[1:])
        upper = t[WINDOW:].reshape((block_count, WINDOW) + t.shape[1:])
        return jnp.concatenate([lower, upper], axis=1)
    query_band = query_rows.astype(jnp.float32).reshape(block_count, WINDOW, kv_heads, group_size, HEAD_DIM)
    key_band = band(key_ext).astype(jnp.float32).reshape(block_count, 2 * WINDOW, kv_heads, HEAD_DIM)
    value_band = band(value_ext).astype(jnp.float32).reshape(block_count, 2 * WINDOW, kv_heads, HEAD_DIM)
    doc_band = band(doc_ext)
    distance = jnp.arange(WINDOW)[:, None] + WINDOW - jnp.arange(2 * WINDOW)[None, :]
    in_window = (distance >= 0) & (distance < WINDOW)
    same_doc = doc_rows.reshape(block_count, WINDOW)[:, :, None] == doc_band[:, None, :]
    keep_mask = in_window[None] & same_doc
    scores = jnp.einsum('nqhgd,nkhd->nhgqk', query_band, key_band) * HEAD_DIM ** (-0.5)
    scores = jnp.where(keep_mask[:, None, None], scores, -jnp.inf)
    sink_logit = sinks.astype(jnp.float32).reshape(kv_heads, group_size)[None, :, :, None, None]
    peak = jnp.maximum(lax.optimization_barrier(jnp.max(scores, axis=-1, keepdims=True)), sink_logit)
    expd = jnp.exp(scores - peak)
    probs = (expd / (lax.optimization_barrier(jnp.sum(expd, axis=-1, keepdims=True)) + jnp.exp(sink_logit - peak))).astype(jnp.bfloat16)
    mixed = jnp.einsum('nhgqk,nkhd->nqhgd', probs.astype(jnp.float32), value_band)
    return mixed.astype(jnp.bfloat16).reshape(row_count, -1)

def convolve(ext_rows, doc_ext, taps):
    center = doc_ext[2:]
    same_one = (doc_ext[1:-1] == center)[:, None]
    same_two = (doc_ext[:-2] == center)[:, None]
    ext32 = ext_rows.astype(jnp.float32)
    result = taps[2] * ext32[2:]
    result = result + jnp.where(same_one, taps[1] * ext32[1:-1], 0.0)
    return result + jnp.where(same_two, taps[0] * ext32[:-2], 0.0)

def reference(queries, keys, values, doc_ids, sinks, residual, out_weight, norm_gain, w_gate, w_value, conv_gate, conv_value, w_down):
    docs_plus = doc_ids + 1
    key_pad = jnp.concatenate([jnp.zeros((WINDOW, KV_W), jnp.bfloat16), keys], axis=0)
    value_pad = jnp.concatenate([jnp.zeros((WINDOW, KV_W), jnp.bfloat16), values], axis=0)
    doc_pad = jnp.concatenate([jnp.zeros((WINDOW,), jnp.int32), docs_plus], axis=0)

    def attend_shard(index):
        start = (index * TOK_SP).astype(jnp.int32)
        return attend(lax.dynamic_slice_in_dim(queries, start, TOK_SP, 0), lax.dynamic_slice_in_dim(key_pad, start, TOK_SP + WINDOW, 0), lax.dynamic_slice_in_dim(value_pad, start, TOK_SP + WINDOW, 0), lax.dynamic_slice_in_dim(docs_plus, start, TOK_SP, 0), lax.dynamic_slice_in_dim(doc_pad, start, TOK_SP + WINDOW, 0), sinks)
    shard_ids = jnp.arange(N_SP, dtype=jnp.int32)
    attn = lax.map(attend_shard, shard_ids).reshape(TOKENS, A_Q)
    proj = jnp.dot(attn, out_weight, preferred_element_type=jnp.float32)
    mid = (residual.astype(jnp.float32) + proj).astype(jnp.bfloat16)
    mid32 = mid.astype(jnp.float32)
    normed = (mid32 * lax.rsqrt(lax.optimization_barrier(jnp.mean(mid32 * mid32, axis=-1, keepdims=True)) + 1e-06) * norm_gain).astype(jnp.bfloat16)
    normed_pad = jnp.concatenate([jnp.zeros((2, D), jnp.bfloat16), normed], axis=0)
    doc_two = jnp.concatenate([jnp.zeros((2,), jnp.int32), docs_plus], axis=0)

    def mlp_shard(index):
        start = (index * TOK_SP).astype(jnp.int32)
        rows_ext = lax.dynamic_slice_in_dim(normed_pad, start, TOK_SP + 2, 0)
        doc_ext = lax.dynamic_slice_in_dim(doc_two, start, TOK_SP + 2, 0)
        gate_pre = jnp.dot(rows_ext, w_gate, preferred_element_type=jnp.float32).astype(jnp.bfloat16)
        value_pre = jnp.dot(rows_ext, w_value, preferred_element_type=jnp.float32).astype(jnp.bfloat16)
        gate_conv = convolve(gate_pre, doc_ext, conv_gate)
        value_conv = convolve(value_pre, doc_ext, conv_value)
        hidden = (jax.nn.silu(gate_conv) * value_conv).astype(jnp.bfloat16)
        return jnp.dot(hidden, w_down, preferred_element_type=jnp.float32)
    mlp = lax.map(mlp_shard, shard_ids).reshape(TOKENS, D)
    return (mid32 + mlp).astype(jnp.bfloat16)
```

```python
import functools

import jax
import jax.numpy as jnp
from jax import lax
from jax.experimental import pallas as pl
from jax.experimental.pallas import tpu as pltpu
from jax.sharding import PartitionSpec as P

HEAD_DIM = 64
WINDOW = 128
MESH = pl.DeviceIdType.MESH
F32 = jnp.float32
BF16 = jnp.bfloat16
NT = (((1,), (1,)), ((), ()))

N_SP = 32
ROWS = 1024
BLK = 256
D = 2048
HID = 1408
HALO = 16
EXT = BLK + HALO
N_SEM = 256


def ceil_dot(a, b):
    return jnp.dot(a, b, preferred_element_type=F32)


def nt_dot(a, b):
    return lax.dot_general(a, b, NT, preferred_element_type=F32)


def kernel(
    q_in,
    kv_in,
    drow_in,
    dcol_in,
    sinks,
    res_in,
    ow_in,
    gain_in,
    wg_in,
    wv_in,
    cg_in,
    cv_in,
    wd_in,
    out,
    q,
    kv,
    kvz,
    drow,
    dcol,
    m1,
    m2,
    att,
    af,
    ow,
    res,
    mid,
    gain,
    nb,
    wu,
    wd,
    pre,
    hid,
    cg,
    cv,
    own,
    pr,
    prf,
    pl_,
    plf,
    pf,
    rl,
    rr,
    tl,
    tr,
    send_sem,
    recv_sem,
    loc_sem,
):
    sp = lax.axis_index("sp")
    x = lax.axis_index("tp")
    c = lax.rem(sp, 2)
    k = lax.div(sp, 2)
    y = lax.rem(k, 4)
    z = lax.div(k, 4)

    def sp_of(zz, yy):
        return (lax.rem(zz + 8, 4) * 4 + lax.rem(yy + 8, 4)) * 2 + c

    def xat(j):
        return lax.rem(x + j + 4, 4)

    def dev(s, t):
        return {"sp": s, "tp": t}

    sp_next = lax.rem(sp + 1, N_SP)
    sp_prev = lax.rem(sp + N_SP - 1, N_SP)
    sib = sp + 1 - 2 * c

    loc = []

    def local(src, dst):
        cp = pltpu.make_async_copy(src, dst, loc_sem.at[len(loc)])
        cp.start()
        loc.append(cp)
        return cp

    piece = (pl.ds(pl.multiple_of(k * 16, 16), 16), pl.ds(pl.multiple_of(c * 1024, 1024), 1024))
    l_kv = local(kv_in, kv.at[pl.ds(WINDOW, ROWS)])
    l_drow = local(drow_in, drow.at[pl.ds(8, 8)])
    l_dcol = local(dcol_in, dcol.at[pl.ds(HALO, ROWS)])
    l_ow = local(ow_in.at[piece], ow.at[x, k, :, piece[1]])
    row64 = pl.ds(pl.multiple_of(sp * 64, 64), 64)
    l_wg = local(wg_in, wu.at[row64, pl.ds(0, HID)])
    l_wv = local(wv_in, wu.at[row64, pl.ds(HID, HID)])
    l_wd = local(wd_in, wd.at[row64])
    l_q = local(q_in, q)
    l_res = local(res_in, res)
    l_gain = local(gain_in, gain)
    l_cg = local(cg_in, cg)
    l_cv = local(cv_in, cv)

    bar = pltpu.get_barrier_semaphore()

    def hello(d):
        pl.semaphore_signal(bar, inc=1, device_id=d, device_id_type=MESH)

    for j in (1, 2, 3):
        hello(dev(sp, xat(j)))
    for dz, dy in ((0, 1), (0, -1), (1, 0), (-1, 0)):
        hello(dev(sp_of(z + dz, y + dy), x))
    hello(dev(sib, x))
    for j in range(4):
        hello(dev(sp_prev, xat(j)))
    pl.semaphore_wait(bar, 12)

    copies = []

    def push(src, dst, d):
        i = len(copies)
        cp = pltpu.make_async_remote_copy(
            src_ref=src,
            dst_ref=dst,
            send_sem=send_sem.at[i],
            recv_sem=recv_sem.at[i],
            device_id=d,
            device_id_type=MESH,
        )
        cp.start()
        copies.append(cp)
        return cp

    l_kv.wait()
    l_drow.wait()
    l_dcol.wait()
    nxt = dev(sp_next, x)
    h_kv = push(kv.at[pl.ds(ROWS, WINDOW)], kv.at[pl.ds(0, WINDOW)], nxt)
    h_drow = push(drow.at[pl.ds(8, 8)], drow.at[pl.ds(0, 8)], nxt)
    h_dcol = push(dcol.at[pl.ds(ROWS, HALO)], dcol.at[pl.ds(0, HALO)], nxt)

    l_ow.wait()
    ow_x = [
        push(ow.at[x, k, :, piece[1]], ow.at[x, k, :, piece[1]], dev(sp, xat(j)))
        for j in (1, 3, 2)
    ]

    def ow_view(half, kk, cc, part):
        col = pl.ds(pl.multiple_of(cc * 1024, 1024), 1024)
        if part is None:
            return ow.at[pl.ds(2 * half, 2), kk, :, col]
        return ow.at[2 * half + part, kk, :, col]

    def wu_view(half, kk, cc, part):
        r = (kk * 2 + cc) * 64
        n = 64 if part is None else 32
        if part == 1:
            r = r + 32
        return wu.at[pl.ds(pl.multiple_of(r, 32), n), pl.ds(half * HID, HID)]

    def wd_view(half, kk, cc, part):
        r = (kk * 2 + cc) * 64 + 32 * half
        n = 32 if part is None else 16
        if part == 1:
            r = r + 16
        return wd.at[pl.ds(pl.multiple_of(r, 16), n)]

    class Gather:
        def __init__(self, view):
            self.view = view
            self.sibs = []
            self.h = [{}, {}]

        def at(self, half, dp, dq, part=None):
            dy, dz = (dp, dq) if half == 0 else (dq, dp)
            kk = lax.rem(z + dz + 8, 4) * 4 + lax.rem(y + dy + 8, 4)
            return self.view(half, kk, c, part)

        def nb(self, half, dp, dq):
            dy, dz = (dp, dq) if half == 0 else (dq, dp)
            return dev(sp_of(z + dz, y + dy), x)

        def go(self, half, ref, d):
            return push(ref, ref, d)

        def share(self, half, ref):
            self.sibs.append(push(ref, ref, dev(sib, x)))

        def s0(self):
            for half in (0, 1):
                h = self.h[half]
                b = self.at(half, 0, 0)
                h["p+"] = self.go(half, b, self.nb(half, 1, 0))
                h["p-"] = self.go(half, b, self.nb(half, -1, 0))
            for half in (0, 1):
                h = self.h[half]
                b = self.at(half, 0, 0)
                h["q+", 0] = self.go(half, b, self.nb(half, 0, 1))
                h["q-", 0] = self.go(half, b, self.nb(half, 0, -1))
                self.share(half, b)

        def s1(self):
            for half in (0, 1):
                h = self.h[half]
                h["p+"].wait_recv()
                h["p+f"] = self.go(half, self.at(half, -1, 0, 0), self.nb(half, 1, 0))
                h["p-"].wait_recv()
                h["p-f"] = self.go(half, self.at(half, 1, 0, 1), self.nb(half, -1, 0))
            for half in (0, 1):
                h = self.h[half]
                for dp in (-1, 1):
                    b = self.at(half, dp, 0)
                    h["q+", dp] = self.go(half, b, self.nb(half, 0, 1))
                    h["q-", dp] = self.go(half, b, self.nb(half, 0, -1))
                    self.share(half, b)

        def s2(self):
            for half in (0, 1):
                h = self.h[half]
                h["p+f"].wait_recv()
                h["p-f"].wait_recv()
                b = self.at(half, 2, 0)
                h["q+", 2] = self.go(half, b, self.nb(half, 0, 1))
                h["q-", 2] = self.go(half, b, self.nb(half, 0, -1))
                self.share(half, b)

        def s3(self, dps=(0, -1, 1, 2)):
            for dp in dps:
                for half in (0, 1):
                    h = self.h[half]
                    h["q+", dp].wait_recv()
                    b = self.at(half, dp, -1)
                    if dp in (0, 1):
                        h["f", dp] = self.go(half, b, self.nb(half, 0, 1))
                    self.share(half, b)
                    h["q-", dp].wait_recv()
                    b = self.at(half, dp, 1)
                    if dp in (2, -1):
                        h["f", dp] = self.go(half, b, self.nb(half, 0, -1))
                    self.share(half, b)

        def s4(self):
            for dp in (0, -1, 1, 2):
                for half in (0, 1):
                    self.h[half]["f", dp].wait_recv()
                    self.share(half, self.at(half, dp, 2))

        def s5(self):
            for s in self.sibs:
                s.wait_recv()

    g_o, g_u, g_d = Gather(ow_view), Gather(wu_view), Gather(wd_view)

    for cp in ow_x:
        cp.wait_recv()
    g_o.s0()
    l_wg.wait()
    l_wv.wait()
    g_u.s0()

    h_kv.wait_recv()
    h_drow.wait_recv()
    h_dcol.wait_recv()
    er = lax.broadcasted_iota(jnp.int32, (128, 2048), 0)
    ec = lax.broadcasted_iota(jnp.int32, (128, 2048), 1)
    sel = (
        ((er >> 6) == (ec >> 10))
        & ((er & 63) == (ec & 63))
        & (((ec >> 8) & 3) == ((ec >> 6) & 3))
    )
    place = jnp.where(sel, 1.0, 0.0).astype(BF16)

    def expand(i, _):
        r = pl.ds(pl.multiple_of(i * 128, 128), 128)
        kvz[r, :] = ceil_dot(kv[r, :], place).astype(BF16)
        return 0

    lax.fori_loop(0, 9, expand, 0)

    first = sp == 0
    t_ids = lax.broadcasted_iota(jnp.int32, (ROWS, 128), 0)
    center = dcol[HALO : HALO + ROWS, :]
    ok1 = (dcol[HALO - 1 : HALO - 1 + ROWS, :] == center) & ((t_ids >= 1) | jnp.logical_not(first))
    ok2 = (dcol[HALO - 2 : HALO - 2 + ROWS, :] == center) & ((t_ids >= 2) | jnp.logical_not(first))
    m1[...] = jnp.where(ok1, 1.0, 0.0)
    m2[...] = jnp.where(ok2, 1.0, 0.0)

    l_q.wait()

    ri = lax.broadcasted_iota(jnp.int32, (128, 128), 0)
    ci = lax.broadcasted_iota(jnp.int32, (128, 128), 1)

    def attend(b):
        r0 = pl.multiple_of(b * 128, 128)
        qb = q[pl.ds(r0, 128), :]
        keys = pl.ds(r0, 256)
        dq = dcol[pl.ds(pl.multiple_of(HALO + b * 128, 8), 128), :]
        k0 = drow[pl.ds(7 + b, 1), :]
        k1 = drow[pl.ds(8 + b, 1), :]
        there = jnp.logical_not(first & (b == 0))
        lower = (dq == k0) & (ci > ri) & there
        upper = (dq == k1) & (ci <= ri)
        keep = jnp.concatenate([lower, upper], axis=1)
        o = jnp.zeros((128, 256), F32)
        for h in range(4):
            s = nt_dot(qb, kvz[keys, h * 256 : (h + 1) * 256]) * (HEAD_DIM**-0.5)
            s = jnp.where(keep, s, -jnp.inf)
            sink = sinks[h]
            peak = jnp.maximum(jnp.max(s, axis=-1, keepdims=True), sink)
            e = jnp.exp(s - peak)
            total = jnp.sum(e, axis=-1, keepdims=True) + jnp.exp(sink - peak)
            p = (e / total).astype(BF16)
            o = o + ceil_dot(p, kvz[keys, 1024 + h * 256 : 1024 + (h + 1) * 256])
        att[pl.ds(r0, 128), :] = o.astype(BF16)

    a2a = {}
    af_col = pl.ds(pl.multiple_of(x * 256, 256), 256)
    for j in (2, 1, 3, 0):
        t = xat(j)

        def two(i, _, t=t):
            attend(t * 2 + i)
            return 0

        lax.fori_loop(0, 2, two, 0)
        rows = att.at[pl.ds(pl.multiple_of(t * 256, 256), 256)]
        if j:
            a2a[j] = push(rows, af.at[:, af_col], dev(sp, t))
        else:
            l_af = local(rows, af.at[:, af_col])
        if j == 1:
            g_o.s1()
        if j == 3:
            g_o.s2()
            g_u.s1()
    g_o.s3()
    g_u.s2()
    l_wd.wait()
    g_d.s0()
    g_o.s4()
    l_af.wait()
    for j in (1, 3, 2):
        a2a[j].wait_recv()
    g_o.s5()

    l_res.wait()
    l_gain.wait()
    l_cg.wait()
    l_cv.wait()

    def project(j, sq):
        col = pl.ds(pl.multiple_of(j * 256, 256), 256)
        w = ow[:, :, :, col].reshape(1024, 256)
        m = res[:, col].astype(F32) + ceil_dot(af[...], w)
        m = m.astype(BF16).astype(F32)
        mid[:, col] = m
        return sq + jnp.sum(m * m, axis=-1, keepdims=True)

    sq = lax.fori_loop(0, D // 256, project, jnp.zeros((BLK, 1), F32))
    inv = lax.rsqrt(sq * (1.0 / D) + 1e-06)
    for j in range(D // 256):
        col = slice(j * 256, (j + 1) * 256)
        nb[x, HALO:EXT, col] = (mid[:, col] * inv * gain[:, col]).astype(BF16)

    slot = xat(1)
    tail = nb.at[x, pl.ds(BLK, HALO)]
    t_sp = jnp.where(x == 3, sp_next, sp)
    tails = [
        push(tail, nb.at[slot, pl.ds(0, HALO)], dev(t_sp, xat(j))) for j in (1, 2, 3)
    ]
    i0 = len(copies)
    copies.append(None)
    tail0 = pltpu.make_async_remote_copy(
        src_ref=tail,
        dst_ref=nb.at[slot, pl.ds(0, HALO)],
        send_sem=send_sem.at[i0],
        recv_sem=recv_sem.at[i0],
        device_id=dev(sp_next, x),
        device_id_type=MESH,
    )
    tail0_local = pltpu.make_async_copy(tail, nb.at[slot, pl.ds(0, HALO)], loc_sem.at[len(loc)])
    loc.append(None)

    @pl.when(x == 3)
    def _():
        tail0.start()

    @pl.when(x != 3)
    def _():
        tail0_local.start()

    def half_of(i, h):
        return nb.at[i, pl.ds(HALO + h * 128, 128)]

    right, left = dev(sp, xat(1)), dev(sp, xat(3))
    n_r0 = push(half_of(x, 0), half_of(x, 0), right)
    n_l1 = push(half_of(x, 1), half_of(x, 1), left)
    n_r1 = push(half_of(x, 1), half_of(x, 1), right)
    n_l0 = push(half_of(x, 0), half_of(x, 0), left)

    g_u.s3()
    g_d.s1()
    n_r0.wait_recv()
    f_r = push(half_of(xat(3), 0), half_of(xat(3), 0), right)
    n_l1.wait_recv()
    f_l = push(half_of(xat(1), 1), half_of(xat(1), 1), left)
    g_u.s4()
    g_d.s2()
    g_u.s5()
    for cp in tails:
        cp.wait_recv()

    @pl.when(x == 3)
    def _():
        tail0.wait()

    @pl.when(x != 3)
    def _():
        tail0_local.wait()

    def up(d):
        def step(j, _):
            col = pl.ds(pl.multiple_of(j * 256, 256), 256)
            pre[:, col] = ceil_dot(nb[d], wu[:, col]).astype(BF16).astype(F32)
            return 0

        lax.fori_loop(0, 2 * HID // 256, step, 0)

    def conv(d):
        def step(j, _):
            gc = pl.ds(pl.multiple_of(j * 128, 128), 128)
            vc = pl.ds(pl.multiple_of(HID + j * 128, 128), 128)
            tg = cg[:, gc]
            tv = cv[:, gc]
            for r in range(0, BLK, 64):
                mr = pl.ds(pl.multiple_of(d * BLK + r, 64), 64)
                k1 = m1[mr, :] > 0.5
                k2 = m2[mr, :] > 0.5

                def taps(t, cc):
                    a = t[2:3] * pre[HALO + r : HALO + r + 64, cc]
                    a = a + jnp.where(k1, t[1:2] * pre[HALO - 1 + r : HALO - 1 + r + 64, cc], 0.0)
                    return a + jnp.where(
                        k2, t[0:1] * pre[HALO - 2 + r : HALO - 2 + r + 64, cc], 0.0
                    )

                g = taps(tg, gc)
                v = taps(tv, vc)
                hid[r : r + 64, gc] = (g / (1.0 + jnp.exp(-g)) * v).astype(BF16)
            return 0

        lax.fori_loop(0, HID // 128, step, 0)

    def down(store):
        def step(j, _):
            r = pl.ds(pl.multiple_of(j * 256, 256), 256)
            store(r, nt_dot(hid[...], wd[r, :]))
            return 0

        lax.fori_loop(0, D // 256, step, 0)

    top, bot = pl.ds(0, 128), pl.ds(128, 128)

    d = xat(1)
    n_l0.wait_recv()
    up(d)
    conv(d)
    g_d.s3()
    g_d.s4()
    g_d.s5()

    def store_r(col, a):
        prf[:, col] = a[:128]
        pr[bot, col] = a[128:].astype(BF16)

    down(store_r)
    s_r1 = push(pr.at[bot], rl.at[bot], right)

    d = xat(3)
    n_r1.wait_recv()
    up(d)
    conv(d)

    def store_l(col, a):
        pl_[top, col] = a[:128].astype(BF16)
        plf[:, col] = a[128:]

    down(store_l)
    s_l0 = push(pl_.at[top], rr.at[top], left)

    d = xat(2)
    f_r.wait_recv()
    f_l.wait_recv()
    up(d)
    conv(d)

    def store_f(col, a):
        pf[:, col] = a.astype(BF16)

    down(store_f)
    s_tr = push(pf.at[top], tl, right)
    s_tl = push(pf.at[bot], tr, left)

    up(x)
    conv(x)

    def store_own(col, a):
        own[:, col] = mid[:, col] + a

    down(store_own)

    s_tr.wait_recv()
    pr[top, :] = (prf[...] + tl[...].astype(F32)).astype(BF16)
    s_r0 = push(pr.at[top], rl.at[top], right)
    s_tl.wait_recv()
    pl_[bot, :] = (plf[...] + tr[...].astype(F32)).astype(BF16)
    s_l1 = push(pl_.at[bot], rr.at[bot], left)

    for cp in (s_r1, s_l0, s_r0, s_l1):
        cp.wait_recv()
    out[...] = (own[...] + rl[...].astype(F32) + rr[...].astype(F32)).astype(BF16)
    for cp in copies:
        if cp is not None:
            cp.wait_send()


def per_device(
    queries,
    keys,
    values,
    doc_ids,
    sinks,
    residual,
    out_weight,
    norm_gain,
    w_gate,
    w_value,
    conv_gate,
    conv_value,
    w_down,
):
    kv = jnp.concatenate([keys, values], axis=1)
    drow = doc_ids.reshape(8, 128)
    dcol = jnp.broadcast_to(doc_ids[:, None], (ROWS, 128))
    wdt = w_down.T
    any_spec = pl.BlockSpec(memory_space=pl.ANY)
    smem = pl.BlockSpec(memory_space=pltpu.SMEM)
    V = pltpu.VMEM
    i32 = jnp.int32
    return pl.pallas_call(
        kernel,
        out_shape=jax.ShapeDtypeStruct((BLK, D), BF16),
        in_specs=[any_spec] * 4 + [smem] + [any_spec] * 8,
        out_specs=pl.BlockSpec(memory_space=pltpu.VMEM),
        scratch_shapes=[
            V((ROWS, 256), BF16),
            V((ROWS + WINDOW, 128), BF16),
            V((ROWS + WINDOW, 2048), BF16),
            V((16, 128), i32),
            V((ROWS + HALO, 128), i32),
            V((ROWS, 128), F32),
            V((ROWS, 128), F32),
            V((ROWS, 256), BF16),
            V((BLK, 1024), BF16),
            V((4, 16, 16, D), BF16),
            V((BLK, D), BF16),
            V((BLK, D), F32),
            V((1, D), F32),
            V((4, EXT, D), BF16),
            V((D, 2 * HID), BF16),
            V((D, HID), BF16),
            V((EXT, 2 * HID), F32),
            V((BLK, HID), BF16),
            V((3, HID), F32),
            V((3, HID), F32),
            V((BLK, D), F32),
            V((BLK, D), BF16),
            V((128, D), F32),
            V((BLK, D), BF16),
            V((128, D), F32),
            V((BLK, D), BF16),
            V((BLK, D), BF16),
            V((BLK, D), BF16),
            V((128, D), BF16),
            V((128, D), BF16),
            pltpu.SemaphoreType.DMA((N_SEM,)),
            pltpu.SemaphoreType.DMA((N_SEM,)),
            pltpu.SemaphoreType.DMA((16,)),
        ],
        compiler_params=pltpu.CompilerParams(
            collective_id=0,
            has_side_effects=True,
            vmem_limit_bytes=67_000_000,
        ),
        cost_estimate=pl.CostEstimate(
            flops=20_000_000_000, bytes_accessed=10_000_000, transcendentals=4_000_000
        ),
    )(
        queries,
        kv,
        drow,
        dcol,
        sinks,
        residual,
        out_weight,
        norm_gain.reshape(1, D),
        w_gate,
        w_value,
        conv_gate,
        conv_value,
        wdt,
    )


def solution(mesh):
    return jax.shard_map(
        per_device,
        mesh=mesh,
        in_specs=(
            P("sp", "tp"),
            P("sp", "tp"),
            P("sp", "tp"),
            P("sp"),
            P("tp"),
            P(("sp", "tp"), None),
            P("tp", None),
            P(),
            P("sp", "tp"),
            P("sp", "tp"),
            P(None, "tp"),
            P(None, "tp"),
            P("tp", "sp"),
        ),
        out_specs=P(("sp", "tp"), None),
        check_vma=False,
    )
```

```python
import functools

import jax
import jax.numpy as jnp
from jax import lax
from jax.experimental import pallas as pl
from jax.experimental.pallas import tpu as pltpu
from jax.sharding import PartitionSpec as P

HEAD_DIM = 64
WINDOW = 128
MESH = pl.DeviceIdType.MESH
F32 = jnp.float32
BF16 = jnp.bfloat16
NT = (((1,), (1,)), ((), ()))

N_SP = 32
ROWS = 1024
BLK = 256
D = 2048
HID = 1408
HALO = 16
EXT = BLK + HALO
N_SEM = 256
RIGHT, LEFT, OWN, ACROSS = 0, 1, 2, 3
SLOT = {0: OWN, 1: RIGHT, 2: ACROSS, 3: LEFT}
TN = (((0,), (0,)), ((), ()))


def ceil_dot(a, b):
    return jnp.dot(a, b, preferred_element_type=F32)


def nt_dot(a, b):
    return lax.dot_general(a, b, NT, preferred_element_type=F32)


def kernel(
    q_in,
    k_in,
    v_in,
    drow_in,
    sinks,
    res_in,
    ow_in,
    gain_in,
    wg_in,
    wv_in,
    cg_in,
    cv_in,
    wd_in,
    out,
    q,
    kvt,
    kvz,
    drow,
    dcol,
    m1,
    m2,
    att,
    af,
    ow,
    res,
    mid,
    gain,
    nb,
    wu,
    wd,
    pre,
    hid,
    cg,
    cv,
    pr,
    prf,
    pl_,
    plf,
    pf,
    rl,
    rr,
    tl,
    tr,
    send_sem,
    recv_sem,
    loc_sem,
):
    sp = lax.axis_index("sp")
    x = lax.axis_index("tp")
    c = lax.rem(sp, 2)
    k = lax.div(sp, 2)
    y = lax.rem(k, 4)
    z = lax.div(k, 4)

    def sp_of(zz, yy):
        return (lax.rem(zz + 8, 4) * 4 + lax.rem(yy + 8, 4)) * 2 + c

    def xat(j):
        return lax.rem(x + j + 4, 4)

    def dev(s, t):
        return {"sp": s, "tp": t}

    sp_next = lax.rem(sp + 1, N_SP)
    sp_prev = lax.rem(sp + N_SP - 1, N_SP)
    sib = sp + 1 - 2 * c
    right, left = dev(sp, xat(1)), dev(sp, xat(3))

    scopes = []

    def phase(name):
        if scopes:
            scopes.pop().__exit__(None, None, None)
        if name:
            scopes.append(jax.named_scope(name))
            scopes[-1].__enter__()

    phase("local")
    bar = pltpu.get_barrier_semaphore()

    def hello(d):
        pl.semaphore_signal(bar, inc=1, device_id=d, device_id_type=MESH)

    for j in (1, 2, 3):
        hello(dev(sp, xat(j)))
    for dz, dy in ((0, 1), (0, -1), (1, 0), (-1, 0)):
        hello(dev(sp_of(z + dz, y + dy), x))
    hello(dev(sib, x))
    for j in range(4):
        hello(dev(sp_prev, xat(j)))

    loc = []

    def local(src, dst):
        cp = pltpu.make_async_copy(src, dst, loc_sem.at[len(loc)])
        cp.start()
        loc.append(cp)
        return cp

    l_k = local(k_in, kvt.at[pl.ds(0, 64), pl.ds(WINDOW, ROWS)])
    l_v = local(v_in, kvt.at[pl.ds(64, 64), pl.ds(WINDOW, ROWS)])
    l_drow = local(drow_in, drow.at[pl.ds(8, 8)])
    l_ow = local(ow_in, ow.at[x])
    row64 = pl.ds(pl.multiple_of(sp * 64, 64), 64)
    l_wg = local(wg_in, wu.at[row64, pl.ds(0, HID)])
    l_wv = local(wv_in, wu.at[row64, pl.ds(HID, HID)])
    l_q = local(q_in, q)
    l_wd = local(wd_in, wd.at[row64])
    l_res = local(res_in, res)
    l_gain = local(gain_in, gain)
    l_cg = local(cg_in, cg)
    l_cv = local(cv_in, cv)

    phase("barrier")
    pl.semaphore_wait(bar, 12)

    phase("send0")
    copies = []

    def push(src, dst, d):
        i = len(copies)
        cp = pltpu.make_async_remote_copy(
            src_ref=src,
            dst_ref=dst,
            send_sem=send_sem.at[i],
            recv_sem=recv_sem.at[i],
            device_id=d,
            device_id_type=MESH,
        )
        cp.start()
        copies.append(cp)
        return cp

    l_k.wait()
    l_v.wait()
    l_drow.wait()
    nxt = dev(sp_next, x)
    h_kv = push(kvt.at[:, pl.ds(ROWS, WINDOW)], kvt.at[:, pl.ds(0, WINDOW)], nxt)
    h_drow = push(drow.at[pl.ds(8, 8)], drow.at[pl.ds(0, 8)], nxt)

    def wu_view(half, kk, cc, part):
        r = (kk * 2 + cc) * 64
        n = 64 if part is None else 32
        if part == 1:
            r = r + 32
        return wu.at[pl.ds(pl.multiple_of(r, 32), n), pl.ds(half * HID, HID)]

    def wd_view(half, kk, cc, part):
        r = (kk * 2 + cc) * 64 + 32 * half
        n = 32 if part is None else 16
        if part == 1:
            r = r + 16
        return wd.at[pl.ds(pl.multiple_of(r, 16), n)]

    def go(ref, d):
        return push(ref, ref, d)

    def yz(half, n):
        dy, dz = (n, 0) if half == 0 else (0, n)
        return dev(sp_of(z + dz, y + dy), x)

    class Gather:
        def __init__(self, view):
            self.view = view
            self.sibs = []
            self.h = [{}, {}]

        def at(self, half, dp, dq, part=None):
            dy, dz = (dp, dq) if half == 0 else (dq, dp)
            kk = lax.rem(z + dz + 8, 4) * 4 + lax.rem(y + dy + 8, 4)
            return self.view(half, kk, c, part)

        def p(self, half, n):
            return yz(half, n)

        def q(self, half, n):
            return yz(1 - half, n)

        def share(self, ref):
            self.sibs.append(go(ref, dev(sib, x)))

        def s0(self):
            for half in (0, 1):
                h = self.h[half]
                b = self.at(half, 0, 0)
                h["p+"] = go(b, self.p(half, 1))
                h["p-"] = go(b, self.p(half, -1))
            self.s1q(0)

        def s1p(self):
            for half in (0, 1):
                h = self.h[half]
                h["p+"].wait_recv()
                h["p+f"] = go(self.at(half, -1, 0, 0), self.p(half, 1))
                h["p-"].wait_recv()
                h["p-f"] = go(self.at(half, 1, 0, 1), self.p(half, -1))

        def s1q(self, dp):
            for half in (0, 1):
                h = self.h[half]
                b = self.at(half, dp, 0)
                h["q+", dp] = go(b, self.q(half, 1))
                h["q-", dp] = go(b, self.q(half, -1))
                self.share(b)

        def s2(self):
            for half in (0, 1):
                h = self.h[half]
                h["p+f"].wait_recv()
                h["p-f"].wait_recv()
            self.s1q(2)

        def s3(self, dps=(0, -1, 1, 2)):
            for dp in dps:
                for half in (0, 1):
                    h = self.h[half]
                    h["q+", dp].wait_recv()
                    b = self.at(half, dp, -1)
                    if dp in (0, 1):
                        h["f", dp] = go(b, self.q(half, 1))
                    self.share(b)
                    h["q-", dp].wait_recv()
                    b = self.at(half, dp, 1)
                    if dp in (2, -1):
                        h["f", dp] = go(b, self.q(half, -1))
                    self.share(b)

        def s4(self):
            for dp in (0, -1, 1, 2):
                for half in (0, 1):
                    self.h[half]["f", dp].wait_recv()
                    self.share(self.at(half, dp, 2))

        def s5(self):
            for s in self.sibs:
                s.wait_recv()

    class GatherOut:
        def __init__(self):
            self.sibs = []
            self.h = {}

        def at(self, j, half, n=0, part=None):
            pos = lax.rem((y if half == 0 else z) + n + 8, 4)
            r = half * 128 + pos * 32
            rows = 32 if part is None else 16
            if part == 1:
                r = r + 16
            cols = pl.ds(pl.multiple_of(c * 1024, 1024), 1024)
            return ow.at[xat(j), pl.ds(pl.multiple_of(r, 16), rows), cols]

        def share(self, ref):
            self.sibs.append(go(ref, dev(sib, x)))

        def spread(self, j, half):
            b = self.at(j, half)
            self.h["+", j, half] = go(b, yz(half, 1))
            self.h["-", j, half] = go(b, yz(half, -1))
            self.share(b)

        def s0(self):
            h = self.h
            h["r", 0] = go(self.at(0, 0), right)
            h["l", 1] = go(self.at(0, 1), left)
            h["r", 1] = go(self.at(0, 1), right)
            h["l", 0] = go(self.at(0, 0), left)

        def s1(self):
            h = self.h
            h["r", 0].wait_recv()
            h["rf"] = go(self.at(3, 0), right)
            self.spread(3, 0)
            h["l", 1].wait_recv()
            h["lf"] = go(self.at(1, 1), left)
            self.spread(1, 1)
            h["r", 1].wait_recv()
            self.spread(3, 1)
            h["l", 0].wait_recv()
            self.spread(1, 0)

        def s2(self):
            self.h["rf"].wait_recv()
            self.spread(2, 0)
            self.h["lf"].wait_recv()
            self.spread(2, 1)

        def s3(self):
            h = self.h
            for j, half in ((3, 0), (1, 1), (3, 1), (1, 0), (2, 0), (2, 1)):
                h["+", j, half].wait_recv()
                h["+f", j, half] = go(self.at(j, half, -1, 0), yz(half, 1))
                self.share(self.at(j, half, -1))
                h["-", j, half].wait_recv()
                h["-f", j, half] = go(self.at(j, half, 1, 1), yz(half, -1))
                self.share(self.at(j, half, 1))

        def s4(self):
            h = self.h
            for j, half in ((3, 0), (1, 1), (3, 1), (1, 0), (2, 0), (2, 1)):
                h["+f", j, half].wait_recv()
                h["-f", j, half].wait_recv()
                self.share(self.at(j, half, 2))

        def s5(self):
            for s in self.sibs:
                s.wait_recv()

    g_o, g_u, g_d = GatherOut(), Gather(wu_view), Gather(wd_view)

    l_ow.wait()
    g_o.s0()
    l_wg.wait()
    l_wv.wait()
    g_u.s0()

    phase("expand")
    er = lax.broadcasted_iota(jnp.int32, (128, 2048), 0)
    ec = lax.broadcasted_iota(jnp.int32, (128, 2048), 1)
    sel = (
        ((er >> 6) == (ec >> 10))
        & ((er & 63) == (ec & 63))
        & (((ec >> 8) & 3) == ((ec >> 6) & 3))
    )
    place = jnp.where(sel, 1.0, 0.0).astype(BF16)

    def expand(i, _):
        r = pl.ds(pl.multiple_of(i * 128, 128), 128)
        kvz[r, :] = lax.dot_general(kvt[:, r], place, TN, preferred_element_type=F32).astype(BF16)
        return 0

    def column(i, _):
        r = pl.ds(pl.multiple_of(HALO + i * 128, 8), 128)
        dcol[r, :] = jnp.broadcast_to(drow[pl.ds(8 + i, 1), :].astype(F32), (128, 128)).T
        return 0

    lax.fori_loop(1, 9, expand, 0)
    lax.fori_loop(0, 8, column, 0)
    phase("o1")
    g_o.s1()
    phase("wait_halo")
    h_kv.wait_recv()
    h_drow.wait_recv()
    phase("masks")
    expand(0, 0)
    ahead = jnp.broadcast_to(drow[7:8, :].astype(F32), (128, 128)).T
    dcol[0:HALO, :] = ahead[128 - HALO :, :]

    first = sp == 0
    t_ids = lax.broadcasted_iota(jnp.int32, (ROWS, 128), 0)
    center = dcol[HALO : HALO + ROWS, :]
    ok1 = (dcol[HALO - 1 : HALO - 1 + ROWS, :] == center) & ((t_ids >= 1) | jnp.logical_not(first))
    ok2 = (dcol[HALO - 2 : HALO - 2 + ROWS, :] == center) & ((t_ids >= 2) | jnp.logical_not(first))
    m1[...] = jnp.where(ok1, 1.0, 0.0)
    m2[...] = jnp.where(ok2, 1.0, 0.0)

    l_q.wait()

    ri = lax.broadcasted_iota(jnp.int32, (128, 128), 0)
    ci = lax.broadcasted_iota(jnp.int32, (128, 128), 1)

    def attend(b):
        r0 = pl.multiple_of(b * 128, 128)
        qb = q[pl.ds(r0, 128), :]
        keys = pl.ds(r0, 256)
        dq = dcol[pl.ds(pl.multiple_of(HALO + b * 128, 8), 128), :]
        k0 = drow[pl.ds(7 + b, 1), :].astype(F32)
        k1 = drow[pl.ds(8 + b, 1), :].astype(F32)
        there = jnp.logical_not(first & (b == 0))
        lower = (dq == k0) & (ci > ri) & there
        upper = (dq == k1) & (ci <= ri)
        keep = jnp.concatenate([lower, upper], axis=1)
        o = jnp.zeros((128, 256), F32)
        for h in range(4):
            s = nt_dot(qb, kvz[keys, h * 256 : (h + 1) * 256]) * (HEAD_DIM**-0.5)
            s = jnp.where(keep, s, -jnp.inf)
            sink = sinks[h]
            peak = jnp.maximum(jnp.max(s, axis=-1, keepdims=True), sink)
            e = jnp.exp(s - peak)
            total = jnp.sum(e, axis=-1, keepdims=True) + jnp.exp(sink - peak)
            p = (e / total).astype(BF16)
            o = o + ceil_dot(p, kvz[keys, 1024 + h * 256 : 1024 + (h + 1) * 256])
        att[pl.ds(r0, 128), :] = o.astype(BF16)

    a2a = {}
    af_col = pl.ds(pl.multiple_of(x * 256, 256), 256)
    for j in (2, 1, 3, 0):
        t = xat(j)

        def two(i, _, t=t):
            attend(t * 2 + i)
            return 0

        phase(f"attend{j}")
        lax.fori_loop(0, 2, two, 0)
        rows = att.at[pl.ds(pl.multiple_of(t * 256, 256), 256)]
        if j:
            a2a[j] = push(rows, af.at[:, af_col], dev(sp, t))
        else:
            l_af = local(rows, af.at[:, af_col])
        if j == 2:
            phase("o2")
            g_o.s2()
        if j == 1:
            phase("u1p")
            g_u.s1p()
            g_u.s1q(-1)
        if j == 3:
            phase("o3")
            g_o.s3()
            phase("u1q")
            g_u.s1q(1)
    phase("o4")
    g_o.s4()
    phase("u2")
    g_u.s2()
    phase("a2a")
    l_af.wait()
    for j in (1, 3, 2):
        a2a[j].wait_recv()
    phase("o5")
    g_o.s5()

    phase("project")
    l_res.wait()
    l_gain.wait()
    l_cg.wait()
    l_cv.wait()

    def project(j, sq):
        col = pl.ds(pl.multiple_of(j * 512, 512), 512)
        w = ow[:, :, col].reshape(1024, 512)
        m = res[:, col].astype(F32) + ceil_dot(af[...], w)
        m = m.astype(BF16).astype(F32)
        mid[:, col] = m
        return sq + jnp.sum(m * m, axis=-1, keepdims=True)

    sq = lax.fori_loop(0, D // 512, project, jnp.zeros((BLK, 1), F32))
    inv = lax.rsqrt(sq * (1.0 / D) + 1e-06)
    for j in range(D // 256):
        col = slice(j * 256, (j + 1) * 256)
        nb[OWN, HALO:EXT, col] = (mid[:, col] * inv * gain[:, col]).astype(BF16)

    phase("send_n")
    tail = nb.at[OWN, pl.ds(BLK, HALO)]
    t_sp = jnp.where(x == 3, sp_next, sp)

    def halo_of(slot):
        return nb.at[slot, pl.ds(0, HALO)]

    tails = [push(tail, halo_of(SLOT[(1 - j) % 4]), dev(t_sp, xat(j))) for j in (1, 2, 3)]
    i0 = len(copies)
    copies.append(None)
    tail0 = pltpu.make_async_remote_copy(
        src_ref=tail,
        dst_ref=halo_of(SLOT[1]),
        send_sem=send_sem.at[i0],
        recv_sem=recv_sem.at[i0],
        device_id=dev(sp_next, x),
        device_id_type=MESH,
    )
    tail0_local = pltpu.make_async_copy(tail, halo_of(SLOT[1]), loc_sem.at[len(loc)])
    loc.append(None)

    @pl.when(x == 3)
    def _():
        tail0.start()

    @pl.when(x != 3)
    def _():
        tail0_local.start()

    def half_of(slot, h):
        return nb.at[slot, pl.ds(HALO + h * 128, 128)]

    n_r0 = push(half_of(OWN, 0), half_of(LEFT, 0), right)
    n_l1 = push(half_of(OWN, 1), half_of(RIGHT, 1), left)
    n_r1 = push(half_of(OWN, 1), half_of(LEFT, 1), right)
    n_l0 = push(half_of(OWN, 0), half_of(RIGHT, 0), left)

    phase("d0")
    l_wd.wait()
    g_d.s0()
    phase("u3")
    g_u.s3()
    phase("d1")
    g_d.s1p()
    g_d.s1q(-1)
    g_d.s1q(1)
    phase("d2")
    g_d.s2()
    phase("n_half")
    n_r0.wait_recv()
    f_r = push(half_of(LEFT, 0), half_of(ACROSS, 0), right)
    n_l1.wait_recv()
    f_l = push(half_of(RIGHT, 1), half_of(ACROSS, 1), left)
    phase("u4")
    g_u.s4()
    phase("d3")
    g_d.s3()
    phase("u5")
    g_u.s5()
    phase("tails")
    for cp in tails:
        cp.wait_recv()

    @pl.when(x == 3)
    def _():
        tail0.wait()

    @pl.when(x != 3)
    def _():
        tail0_local.wait()

    def up(slot, n):
        rows = nb[slot : slot + n].reshape(n * EXT, D)
        for h in (0, 1):
            col = pl.ds(h * HID, HID)
            pre[: n * EXT, col] = ceil_dot(rows, wu[:, col]).astype(BF16).astype(F32)

    def conv(slot, base, d):
        def step(j, _):
            gc = pl.ds(pl.multiple_of(j * 128, 128), 128)
            vc = pl.ds(pl.multiple_of(HID + j * 128, 128), 128)
            tg = cg[:, gc]
            tv = cv[:, gc]
            for r in range(0, BLK, 64):
                mr = pl.ds(pl.multiple_of(d * BLK + r, 64), 64)
                k1 = m1[mr, :] > 0.5
                k2 = m2[mr, :] > 0.5
                r0 = base * EXT + HALO + r

                def taps(t, cc):
                    a = t[2:3] * pre[r0 : r0 + 64, cc]
                    a = a + jnp.where(k1, t[1:2] * pre[r0 - 1 : r0 + 63, cc], 0.0)
                    return a + jnp.where(k2, t[0:1] * pre[r0 - 2 : r0 + 62, cc], 0.0)

                g = taps(tg, gc)
                v = taps(tv, vc)
                hid[slot, r : r + 64, gc] = (g / (1.0 + jnp.exp(-g)) * v).astype(BF16)
            return 0

        lax.fori_loop(0, HID // 128, step, 0)

    chunks = (pl.ds(0, 1024), pl.ds(1024, 1024))
    top, bot = pl.ds(0, 128), pl.ds(128, 128)

    phase("up0")
    up(OWN, 1)
    phase("conv0")
    conv(OWN, 0, x)
    phase("d4")
    g_d.s4()

    phase("wait_n1")
    n_l0.wait_recv()
    n_r1.wait_recv()
    phase("up13")
    up(RIGHT, 2)
    phase("conv13")
    conv(RIGHT, 0, xat(1))
    conv(LEFT, 1, xat(3))
    phase("d5")
    g_d.s5()
    phase("down13")
    s_one, s_two, s_three = [], [], []
    for col in chunks:
        a = nt_dot(hid[0:2].reshape(2 * BLK, HID), wd[col, :])
        prf[:, col] = a[:128]
        pr[bot, col] = a[128:256].astype(BF16)
        pl_[top, col] = a[256:384].astype(BF16)
        plf[:, col] = a[384:]
        s_one.append(push(pr.at[bot, col], rl.at[bot, col], right))
        s_one.append(push(pl_.at[top, col], rr.at[top, col], left))

    phase("wait_n2")
    f_r.wait_recv()
    f_l.wait_recv()
    phase("up2")
    up(ACROSS, 1)
    phase("conv2")
    conv(ACROSS, 0, xat(2))
    phase("down2")
    for col in chunks:
        pf[:, col] = nt_dot(hid[ACROSS], wd[col, :]).astype(BF16)
        s_two.append(
            (
                push(pf.at[top, col], tl.at[:, col], right),
                push(pf.at[bot, col], tr.at[:, col], left),
            )
        )

    phase("down0")
    for col in chunks:
        mid[:, col] += nt_dot(hid[OWN], wd[col, :])

    for i, col in enumerate(chunks):
        phase("wait_t")
        s_two[i][0].wait_recv()
        pr[top, col] = (prf[:, col] + tl[:, col].astype(F32)).astype(BF16)
        s_three.append(push(pr.at[top, col], rl.at[top, col], right))
        s_two[i][1].wait_recv()
        pl_[bot, col] = (plf[:, col] + tr[:, col].astype(F32)).astype(BF16)
        s_three.append(push(pl_.at[bot, col], rr.at[bot, col], left))

    phase("wait_s1")
    for cp in s_one:
        cp.wait_recv()
    for i, col in enumerate(chunks):
        phase("wait_s3")
        s_three[2 * i].wait_recv()
        s_three[2 * i + 1].wait_recv()
        phase("final")
        out[:, col] = (mid[:, col] + rl[:, col].astype(F32) + rr[:, col].astype(F32)).astype(BF16)
    phase("wait_sends")
    for cp in copies:
        if cp is not None:
            cp.wait_send()
    phase(None)


def per_device(
    queries,
    keys,
    values,
    doc_ids,
    sinks,
    residual,
    out_weight,
    norm_gain,
    w_gate,
    w_value,
    conv_gate,
    conv_value,
    w_down,
):
    drow = doc_ids.reshape(8, 128)
    wdt = w_down.T
    any_spec = pl.BlockSpec(memory_space=pl.ANY)
    smem = pl.BlockSpec(memory_space=pltpu.SMEM)
    V = pltpu.VMEM
    i32 = jnp.int32
    return pl.pallas_call(
        kernel,
        out_shape=jax.ShapeDtypeStruct((BLK, D), BF16),
        in_specs=[any_spec] * 4 + [smem] + [any_spec] * 8,
        out_specs=pl.BlockSpec(memory_space=pltpu.VMEM),
        scratch_shapes=[
            V((ROWS, 256), BF16),
            V((128, ROWS + WINDOW), BF16),
            V((ROWS + WINDOW, 2048), BF16),
            V((16, 128), i32),
            V((ROWS + HALO, 128), F32),
            V((ROWS, 128), F32),
            V((ROWS, 128), F32),
            V((ROWS, 256), BF16),
            V((BLK, 1024), BF16),
            V((4, 256, D), BF16),
            V((BLK, D), BF16),
            V((BLK, D), F32),
            V((1, D), F32),
            V((4, EXT, D), BF16),
            V((D, 2 * HID), BF16),
            V((D, HID), BF16),
            V((2 * EXT, 2 * HID), F32),
            V((4, BLK, HID), BF16),
            V((3, HID), F32),
            V((3, HID), F32),
            V((BLK, D), BF16),
            V((128, D), F32),
            V((BLK, D), BF16),
            V((128, D), F32),
            V((BLK, D), BF16),
            V((BLK, D), BF16),
            V((BLK, D), BF16),
            V((128, D), BF16),
            V((128, D), BF16),
            pltpu.SemaphoreType.DMA((N_SEM,)),
            pltpu.SemaphoreType.DMA((N_SEM,)),
            pltpu.SemaphoreType.DMA((16,)),
        ],
        compiler_params=pltpu.CompilerParams(
            collective_id=0,
            has_side_effects=True,
            vmem_limit_bytes=67_000_000,
        ),
        cost_estimate=pl.CostEstimate(
            flops=20_000_000_000, bytes_accessed=10_000_000, transcendentals=4_000_000
        ),
    )(
        queries,
        keys.T,
        values.T,
        drow,
        sinks,
        residual,
        out_weight,
        norm_gain.reshape(1, D),
        w_gate,
        w_value,
        conv_gate,
        conv_value,
        wdt,
    )


def solution(mesh):
    return jax.shard_map(
        per_device,
        mesh=mesh,
        in_specs=(
            P("sp", "tp"),
            P("sp", "tp"),
            P("sp", "tp"),
            P("sp"),
            P("tp"),
            P(("sp", "tp"), None),
            P("tp", None),
            P(),
            P("sp", "tp"),
            P("sp", "tp"),
            P(None, "tp"),
            P(None, "tp"),
            P("tp", "sp"),
        ),
        out_specs=P(("sp", "tp"), None),
        check_vma=False,
    )
```

```python
import functools

import jax
import jax.numpy as jnp
from jax import lax
from jax.experimental import pallas as pl
from jax.experimental.pallas import tpu as pltpu
from jax.sharding import PartitionSpec as P

HEAD_DIM = 64
WINDOW = 128
MESH = pl.DeviceIdType.MESH
F32 = jnp.float32
BF16 = jnp.bfloat16
NT = (((1,), (1,)), ((), ()))

N_SP = 32
ROWS = 1024
BLK = 256
D = 2048
HID = 1408
HALO = 8
HALF = BLK // 2
EXT = HALF + HALO
PAIR = 2 * EXT
N_SEND, N_RECV = 40, 64
R1, L0, R0, L1, O0, O1, A0, A1 = range(8)
FIRST = {0: O0, 1: R0, 2: A0, 3: L0}
TN = (((0,), (0,)), ((), ()))


def ceil_dot(a, b):
    return jnp.dot(a, b, preferred_element_type=F32)


def nt_dot(a, b):
    return lax.dot_general(a, b, NT, preferred_element_type=F32)


def kernel(
    q_in,
    k_in,
    v_in,
    drow_in,
    sinks,
    res_in,
    ow_in,
    gain_in,
    wg_in,
    wv_in,
    cg_in,
    cv_in,
    wd_in,
    out,
    q,
    kvt,
    kvz,
    drow,
    dcol,
    m1,
    m2,
    att,
    af,
    ow,
    res,
    mid,
    gain,
    nb,
    wu,
    wd,
    pre,
    hid,
    cg,
    cv,
    s1,
    s2,
    s3,
    p3,
    rl,
    rr,
    tl,
    tr,
    send_sem,
    recv_sem,
    loc_sem,
):
    sp = lax.axis_index("sp")
    x = lax.axis_index("tp")
    c = lax.rem(sp, 2)
    k = lax.div(sp, 2)
    y = lax.rem(k, 4)
    z = lax.div(k, 4)

    def sp_of(zz, yy):
        return (lax.rem(zz + 8, 4) * 4 + lax.rem(yy + 8, 4)) * 2 + c

    def xat(j):
        return lax.rem(x + j + 4, 4)

    def dev(s, t):
        return {"sp": s, "tp": t}

    sp_next = lax.rem(sp + 1, N_SP)
    sp_prev = lax.rem(sp + N_SP - 1, N_SP)
    sib = sp + 1 - 2 * c
    right, left = dev(sp, xat(1)), dev(sp, xat(3))

    scopes = []

    def phase(name):
        if scopes:
            scopes.pop().__exit__(None, None, None)
        if name:
            scopes.append(jax.named_scope(name))
            scopes[-1].__enter__()

    phase("local")
    bar = pltpu.get_barrier_semaphore()

    def hello(d):
        pl.semaphore_signal(bar, inc=1, device_id=d, device_id_type=MESH)

    for j in (1, 2, 3):
        hello(dev(sp, xat(j)))
    for dz, dy in ((0, 1), (0, -1), (1, 0), (-1, 0)):
        hello(dev(sp_of(z + dz, y + dy), x))
    hello(dev(sib, x))
    for j in range(4):
        hello(dev(sp_prev, xat(j)))

    loc = []

    def local(src, dst):
        cp = pltpu.make_async_copy(src, dst, loc_sem.at[len(loc)])
        cp.start()
        loc.append(cp)
        return cp

    l_k = local(k_in, kvt.at[pl.ds(0, 64), pl.ds(WINDOW, ROWS)])
    l_v = local(v_in, kvt.at[pl.ds(64, 64), pl.ds(WINDOW, ROWS)])
    l_drow = local(drow_in, drow.at[pl.ds(8, 8)])
    l_ow = local(ow_in, ow.at[x])
    row64 = pl.ds(pl.multiple_of(sp * 64, 64), 64)
    l_wg = local(wg_in, wu.at[row64, pl.ds(0, HID)])
    l_wv = local(wv_in, wu.at[row64, pl.ds(HID, HID)])
    l_q = local(q_in, q)
    l_wd = local(wd_in, wd.at[row64])
    l_res = local(res_in, res)
    l_gain = local(gain_in, gain)
    l_cg = local(cg_in, cg)
    l_cv = local(cv_in, cv)

    er = lax.broadcasted_iota(jnp.int32, (128, 2048), 0)
    ec = lax.broadcasted_iota(jnp.int32, (128, 2048), 1)
    sel = (
        ((er >> 6) == (ec >> 10))
        & ((er & 63) == (ec & 63))
        & (((ec >> 8) & 3) == ((ec >> 6) & 3))
    )
    place = jnp.where(sel, 1.0, 0.0).astype(BF16)

    def column(i, _):
        r = pl.ds(pl.multiple_of(HALO + i * 128, 8), 128)
        dcol[r, :] = jnp.broadcast_to(drow[pl.ds(8 + i, 1), :].astype(F32), (128, 128)).T
        return 0

    l_drow.wait()
    lax.fori_loop(0, 8, column, 0)

    phase("barrier")
    pl.semaphore_wait(bar, 12)

    phase("send0")
    copies = []
    used = {"s": 0, "r": 0}

    def new(kind):
        used[kind] += 1
        return (send_sem if kind == "s" else recv_sem).at[used[kind] - 1]

    def push(src, dst, d, ss=None, rs=None):
        cp = pltpu.make_async_remote_copy(
            src_ref=src,
            dst_ref=dst,
            send_sem=new("s") if ss is None else ss,
            recv_sem=new("r") if rs is None else rs,
            device_id=d,
            device_id_type=MESH,
        )
        cp.start()
        if ss is None:
            copies.append(cp)
        return cp

    def wait_all(sem, view):
        pltpu.make_async_copy(view, view, sem).wait()

    l_k.wait()
    l_v.wait()
    nxt = dev(sp_next, x)
    h_kv = push(kvt.at[:, pl.ds(ROWS, WINDOW)], kvt.at[:, pl.ds(0, WINDOW)], nxt)
    h_drow = push(drow.at[pl.ds(8, 8)], drow.at[pl.ds(0, 8)], nxt)

    def wu_view(half, kk, cc, part):
        r = (kk * 2 + cc) * 64
        n = 64 if part is None else 32
        if part == 1:
            r = r + 32
        return wu.at[pl.ds(pl.multiple_of(r, 32), n), pl.ds(half * HID, HID)]

    def wd_view(half, kk, cc, part):
        r = (kk * 2 + cc) * 64 + 32 * half
        n = 32 if part is None else 16
        if part == 1:
            r = r + 16
        return wd.at[pl.ds(pl.multiple_of(r, 16), n)]

    def yz(half, n):
        dy, dz = (n, 0) if half == 0 else (0, n)
        return dev(sp_of(z + dz, y + dy), x)

    class Group:
        def __init__(self, size):
            self.size = size
            self.ss = new("s")
            self.sent = 0
            self.sem = {}
            self.due = {}

        def go(self, key, ref, units, d):
            if key not in self.sem:
                self.sem[key] = new("r")
                self.due[key] = 0
            push(ref, ref, d, self.ss, self.sem[key])
            self.due[key] += units
            self.sent += units

        def come(self, key):
            wait_all(self.sem[key], self.size(self.due[key]))

        def share(self, ref, units=2):
            self.go("sib", ref, units, dev(sib, x))

        def s5(self):
            self.come("sib")

        def gone(self):
            wait_all(self.ss, self.size(self.sent))

    class Gather(Group):
        def __init__(self, view, size):
            super().__init__(size)
            self.view = view

        def at(self, half, dp, dq, part=None):
            dy, dz = (dp, dq) if half == 0 else (dq, dp)
            kk = lax.rem(z + dz + 8, 4) * 4 + lax.rem(y + dy + 8, 4)
            return self.view(half, kk, c, part)

        def p(self, half, n):
            return yz(half, n)

        def q(self, half, n):
            return yz(1 - half, n)

        def s0p(self):
            for half in (0, 1):
                b = self.at(half, 0, 0)
                self.go("p", b, 2, self.p(half, 1))
                self.go("p", b, 2, self.p(half, -1))

        def s1p(self):
            self.come("p")
            for half in (0, 1):
                self.go("pf", self.at(half, -1, 0, 0), 1, self.p(half, 1))
                self.go("pf", self.at(half, 1, 0, 1), 1, self.p(half, -1))

        def s1q(self, dp):
            for half in (0, 1):
                b = self.at(half, dp, 0)
                self.go(("q", dp), b, 2, self.q(half, 1))
                self.go(("q", dp), b, 2, self.q(half, -1))
                self.share(b)

        def s2(self):
            self.come("pf")
            self.s1q(2)

        def s3(self, dps):
            for dp in dps:
                self.come(("q", dp))
                for half in (0, 1):
                    lo, hi = self.at(half, dp, -1), self.at(half, dp, 1)
                    if dp in (0, 1):
                        self.go("f", lo, 2, self.q(half, 1))
                    else:
                        self.go("f", hi, 2, self.q(half, -1))
                    self.share(lo)
                    self.share(hi)

        def s4(self):
            self.come("f")
            for dp in (0, -1, 1, 2):
                for half in (0, 1):
                    self.share(self.at(half, dp, 2))

    class GatherOut(Group):
        def at(self, j, par, r, n):
            r = lax.rem(y + z + par, 2) * 128 + r
            cols = pl.ds(pl.multiple_of(c * 1024, 1024), 1024)
            return ow.at[xat(j), pl.ds(pl.multiple_of(r, 32), n), cols]

        def piece(self, j, half):
            return self.at(j, 0, half * 64, 64)

        def spread(self, j, half, n):
            for i in (0, 1):
                self.go(("y", n), self.at(j, 0, half * 64 + i * 32, 32), 2, yz(half, 1 - 2 * i))
            self.share(self.piece(j, half), 4)

        def s0(self):
            self.go("x0", self.piece(0, 0), 4, right)
            self.go("x0", self.piece(0, 1), 4, left)
            self.go("x1", self.piece(0, 1), 4, right)
            self.go("x1", self.piece(0, 0), 4, left)

        def s1a(self):
            self.come("x0")
            self.go("xf", self.piece(3, 0), 4, right)
            self.go("xf", self.piece(1, 1), 4, left)
            self.spread(3, 0, 0)
            self.spread(1, 1, 0)

        def s1b(self):
            self.come("x1")
            self.spread(3, 1, 1)
            self.spread(1, 0, 1)

        def s2(self):
            self.come("xf")
            self.spread(2, 0, 2)
            self.spread(2, 1, 2)

        def s4(self, n):
            self.come(("y", n))
            for j, half in (((3, 0), (1, 1)), ((3, 1), (1, 0)), ((2, 0), (2, 1)))[n]:
                self.share(self.at(j, 1, half * 64, 64), 4)

    def ow_size(n):
        for quarters in (1, 2, 3, 4):
            if n * 8 % quarters == 0 and n * 8 // quarters <= 256:
                return ow.at[pl.ds(0, quarters), pl.ds(0, n * 8 // quarters)]

    g_o = GatherOut(ow_size)
    g_u = Gather(wu_view, lambda n: wu.at[pl.ds(0, 16 * n)])
    g_d = Gather(wd_view, lambda n: wd.at[pl.ds(0, 16 * n)])

    l_ow.wait()
    g_o.s0()
    l_wg.wait()
    l_wv.wait()
    g_u.s0p()

    phase("expand")

    def expand(i, _):
        r = pl.ds(pl.multiple_of(i * 128, 128), 128)
        kvz[r, :] = lax.dot_general(kvt[:, r], place, TN, preferred_element_type=F32).astype(BF16)
        return 0

    lax.fori_loop(1, 9, expand, 0)
    phase("o1")
    g_o.s1a()
    phase("wait_halo")
    h_kv.wait_recv()
    h_drow.wait_recv()
    phase("masks")
    expand(0, 0)
    ahead = jnp.broadcast_to(drow[7:8, :].astype(F32), (128, 128)).T
    dcol[0:HALO, :] = ahead[128 - HALO :, :]

    first = sp == 0
    t_ids = lax.broadcasted_iota(jnp.int32, (ROWS, 128), 0)
    center = dcol[HALO : HALO + ROWS, :]
    ok1 = (dcol[HALO - 1 : HALO - 1 + ROWS, :] == center) & ((t_ids >= 1) | jnp.logical_not(first))
    ok2 = (dcol[HALO - 2 : HALO - 2 + ROWS, :] == center) & ((t_ids >= 2) | jnp.logical_not(first))
    m1[...] = jnp.where(ok1, 1.0, 0.0)
    m2[...] = jnp.where(ok2, 1.0, 0.0)

    l_q.wait()

    ri = lax.broadcasted_iota(jnp.int32, (128, 128), 0)
    ci = lax.broadcasted_iota(jnp.int32, (128, 128), 1)

    def attend(b):
        r0 = pl.multiple_of(b * 128, 128)
        qb = q[pl.ds(r0, 128), :]
        keys = pl.ds(r0, 256)
        dq = dcol[pl.ds(pl.multiple_of(HALO + b * 128, 8), 128), :]
        k0 = drow[pl.ds(7 + b, 1), :].astype(F32)
        k1 = drow[pl.ds(8 + b, 1), :].astype(F32)
        there = jnp.logical_not(first & (b == 0))
        lower = (dq == k0) & (ci > ri) & there
        upper = (dq == k1) & (ci <= ri)
        keep = jnp.concatenate([lower, upper], axis=1)
        o = jnp.zeros((128, 256), F32)
        for h in range(4):
            s = nt_dot(qb, kvz[keys, h * 256 : (h + 1) * 256]) * (HEAD_DIM**-0.5)
            s = jnp.where(keep, s, -jnp.inf)
            sink = sinks[h]
            peak = jnp.maximum(jnp.max(s, axis=-1, keepdims=True), sink)
            e = jnp.exp(s - peak)
            total = jnp.sum(e, axis=-1, keepdims=True) + jnp.exp(sink - peak)
            p = (e / total).astype(BF16)
            o = o + ceil_dot(p, kvz[keys, 1024 + h * 256 : 1024 + (h + 1) * 256])
        att[pl.ds(r0, 128), :] = o.astype(BF16)

    a2a = {}
    af_col = pl.ds(pl.multiple_of(x * 256, 256), 256)
    for j in (2, 1, 3, 0):
        t = xat(j)

        def two(i, _, t=t):
            attend(t * 2 + i)
            return 0

        phase(f"attend{j}")
        lax.fori_loop(0, 2, two, 0)
        rows = att.at[pl.ds(pl.multiple_of(t * 256, 256), 256)]
        if j:
            a2a[j] = push(rows, af.at[:, af_col], dev(sp, t))
        else:
            l_af = local(rows, af.at[:, af_col])
        if j == 2:
            phase("d0p")
            l_wd.wait()
            g_d.s0p()
        if j == 1:
            phase("o1b")
            g_o.s1b()
            g_u.s1p()
        if j == 3:
            phase("o2")
            g_o.s2()
            g_u.s1q(0)
    phase("u1")
    g_u.s1q(-1)
    g_u.s1q(1)
    g_o.s4(0)
    phase("a2a")
    l_af.wait()
    for j in (1, 3, 2):
        a2a[j].wait_recv()
    phase("o4")
    g_o.s4(1)
    g_o.s4(2)
    phase("u2")
    g_u.s2()
    phase("o5")
    g_o.s5()

    phase("project")
    l_res.wait()
    l_gain.wait()
    l_cg.wait()
    l_cv.wait()

    def project(j, sq):
        col = pl.ds(pl.multiple_of(j * 512, 512), 512)
        w = ow[:, :, col].reshape(1024, 512)
        m = res[:, col].astype(F32) + ceil_dot(af[...], w)
        m = m.astype(BF16).astype(F32)
        mid[:, col] = m
        return sq + jnp.sum(m * m, axis=-1, keepdims=True)

    sq = lax.fori_loop(0, D // 512, project, jnp.zeros((BLK, 1), F32))
    inv = lax.rsqrt(sq * (1.0 / D) + 1e-06)
    for h in (0, 1):
        r = slice(h * HALF, (h + 1) * HALF)
        for j in range(D // 512):
            col = slice(j * 512, (j + 1) * 512)
            n = (mid[r, col] * inv[r] * gain[:, col]).astype(BF16)
            nb[O0 + h, HALO:EXT, col] = n
            if h == 0:
                nb[O1, 0:HALO, col] = n[HALF - HALO :]

    phase("send_n")

    def rows_of(i):
        return nb.at[i, pl.ds(HALO, HALF)]

    def halo_of(i):
        return nb.at[i, pl.ds(0, HALO)]

    tail = nb.at[O1, pl.ds(HALF, HALO)]
    t_sp = jnp.where(x == 3, sp_next, sp)
    n_mid = push(halo_of(O1), halo_of(R1), left)
    tails = [push(tail, halo_of(FIRST[(1 - j) % 4]), dev(t_sp, xat(j))) for j in (1, 3)]
    n_r0 = push(rows_of(O0), rows_of(L0), right)
    n_l1 = push(rows_of(O1), rows_of(R1), left)
    tails.append(push(tail, halo_of(FIRST[3]), dev(t_sp, xat(2))))
    tail0 = pltpu.make_async_remote_copy(
        src_ref=tail,
        dst_ref=halo_of(R0),
        send_sem=new("s"),
        recv_sem=new("r"),
        device_id=dev(sp_next, x),
        device_id_type=MESH,
    )
    tail0_local = pltpu.make_async_copy(tail, halo_of(R0), loc_sem.at[len(loc)])
    loc.append(None)

    @pl.when(x == 3)
    def _():
        tail0.start()

    @pl.when(x != 3)
    def _():
        tail0_local.start()

    n_r1 = push(rows_of(O1), rows_of(L1), right)
    n_l0 = push(rows_of(O0), rows_of(R0), left)

    phase("u3a")
    g_u.s3((0,))
    g_d.s1p()
    phase("u3b")
    g_u.s3((-1,))
    g_d.s1q(0)
    g_d.s1q(-1)
    phase("u3c")
    g_u.s3((1,))
    g_d.s1q(1)
    phase("u3d")
    g_u.s3((2,))
    phase("n_half")
    n_r0.wait_recv()
    f_r = push(rows_of(L0), rows_of(A0), right)
    n_l1.wait_recv()
    f_l = push(rows_of(R1), rows_of(A1), left)
    phase("d2")
    g_d.s2()
    phase("d3a")
    g_d.s3((0,))
    phase("u4")
    g_u.s4()
    phase("d3b")
    g_d.s3((-1, 1))
    phase("d3c")
    g_d.s3((2,))
    phase("u5")
    g_u.s5()
    phase("tails")
    n_mid.wait_recv()
    for cp in tails:
        cp.wait_recv()

    @pl.when(x == 3)
    def _():
        tail0.wait()

    @pl.when(x != 3)
    def _():
        tail0_local.wait()

    def up(i):
        rows = nb[i : i + 2].reshape(PAIR, D)
        for h in (0, 1):
            col = pl.ds(h * HID, HID)
            pre[:, col] = ceil_dot(rows, wu[:, col]).astype(BF16).astype(F32)

    def conv(i, blocks):
        def step(j, _):
            gc = pl.ds(pl.multiple_of(j * 128, 128), 128)
            vc = pl.ds(pl.multiple_of(HID + j * 128, 128), 128)
            tg = cg[:, gc]
            tv = cv[:, gc]
            for n, (d, h) in enumerate(blocks):
                for r in range(0, HALF, 64):
                    mr = pl.ds(pl.multiple_of(d * BLK + h * HALF + r, 64), 64)
                    k1 = m1[mr, :] > 0.5
                    k2 = m2[mr, :] > 0.5
                    r0 = n * EXT + HALO + r

                    def taps(t, cc):
                        a = t[2:3] * pre[r0 : r0 + 64, cc]
                        a = a + jnp.where(k1, t[1:2] * pre[r0 - 1 : r0 + 63, cc], 0.0)
                        return a + jnp.where(k2, t[0:1] * pre[r0 - 2 : r0 + 62, cc], 0.0)

                    g = taps(tg, gc)
                    v = taps(tv, vc)
                    o = n * HALF + r
                    hid[i // 2, o : o + 64, gc] = (g / (1.0 + jnp.exp(-g)) * v).astype(BF16)
            return 0

        lax.fori_loop(0, HID // 128, step, 0)

    chunks = (pl.ds(0, 1024), pl.ds(1024, 1024))
    top, bot = pl.ds(0, HALF), pl.ds(HALF, HALF)

    def down(i, col):
        return nt_dot(hid[i // 2], wd[col, :])

    phase("up0")
    up(O0)
    phase("conv0")
    conv(O0, ((x, 0), (x, 1)))

    phase("up1")
    up(R1)
    phase("d4")
    g_d.s4()
    phase("conv1")
    conv(R1, ((xat(1), 1), (xat(3), 0)))
    phase("d5")
    g_d.s5()
    phase("down1")
    s_one, s_two, s_three = [], [], []
    for col in chunks:
        a = down(R1, col)
        s1[:, col] = a.astype(BF16)
        s_one.append(push(s1.at[top, col], rl.at[bot, col], right))
        s_one.append(push(s1.at[bot, col], rr.at[top, col], left))

    phase("wait_n2")
    f_r.wait_recv()
    f_l.wait_recv()
    nb[A1, 0:HALO, :] = nb[A0, HALF:EXT, :]
    phase("up2")
    up(A0)
    phase("conv2")
    conv(A0, ((xat(2), 0), (xat(2), 1)))
    phase("down2")
    for col in chunks:
        s2[:, col] = down(A0, col).astype(BF16)
        s_two.append(
            (
                push(s2.at[top, col], tl.at[:, col], right),
                push(s2.at[bot, col], tr.at[:, col], left),
            )
        )

    phase("wait_n1")
    n_l0.wait_recv()
    n_r1.wait_recv()
    nb[L1, 0:HALO, :] = nb[L0, HALF:EXT, :]
    phase("up3")
    up(R0)
    phase("conv3")
    conv(R0, ((xat(1), 0), (xat(3), 1)))
    phase("down3")
    for col in chunks:
        p3[:, col] = down(R0, col)

    def finish(i, col):
        s_two[i][0].wait_recv()
        s3[top, col] = (p3[top, col] + tl[:, col].astype(F32)).astype(BF16)
        s_three.append(push(s3.at[top, col], rl.at[top, col], right))
        s_two[i][1].wait_recv()
        s3[bot, col] = (p3[bot, col] + tr[:, col].astype(F32)).astype(BF16)
        s_three.append(push(s3.at[bot, col], rr.at[bot, col], left))

    phase("down0")
    for col in chunks:
        mid[:, col] += down(O0, col)
    for i, col in enumerate(chunks):
        phase("wait_t")
        finish(i, col)

    phase("wait_s1")
    for cp in s_one:
        cp.wait_recv()
    for i, col in enumerate(chunks):
        phase("wait_s3")
        s_three[2 * i].wait_recv()
        s_three[2 * i + 1].wait_recv()
        phase("final")
        out[:, col] = (mid[:, col] + rl[:, col].astype(F32) + rr[:, col].astype(F32)).astype(BF16)
    phase("wait_sends")
    for cp in copies:
        cp.wait_send()
    for g in (g_o, g_u, g_d):
        g.gone()
    phase(None)
    assert used["s"] <= N_SEND and used["r"] <= N_RECV, used


def per_device(
    queries,
    keys,
    values,
    doc_ids,
    sinks,
    residual,
    out_weight,
    norm_gain,
    w_gate,
    w_value,
    conv_gate,
    conv_value,
    w_down,
):
    drow = doc_ids.reshape(8, 128)
    wdt = w_down.T
    any_spec = pl.BlockSpec(memory_space=pl.ANY)
    smem = pl.BlockSpec(memory_space=pltpu.SMEM)
    V = pltpu.VMEM
    i32 = jnp.int32
    return pl.pallas_call(
        kernel,
        out_shape=jax.ShapeDtypeStruct((BLK, D), BF16),
        in_specs=[any_spec] * 4 + [smem] + [any_spec] * 8,
        out_specs=pl.BlockSpec(memory_space=pltpu.VMEM),
        scratch_shapes=[
            V((ROWS, 256), BF16),
            V((128, ROWS + WINDOW), BF16),
            V((ROWS + WINDOW, 2048), BF16),
            V((16, 128), i32),
            V((ROWS + HALO, 128), F32),
            V((ROWS, 128), F32),
            V((ROWS, 128), F32),
            V((ROWS, 256), BF16),
            V((BLK, 1024), BF16),
            V((4, 256, D), BF16),
            V((BLK, D), BF16),
            V((BLK, D), F32),
            V((1, D), F32),
            V((8, EXT, D), BF16),
            V((D, 2 * HID), BF16),
            V((D, HID), BF16),
            V((PAIR, 2 * HID), F32),
            V((4, BLK, HID), BF16),
            V((3, HID), F32),
            V((3, HID), F32),
            V((BLK, D), BF16),
            V((BLK, D), BF16),
            V((BLK, D), BF16),
            V((BLK, D), F32),
            V((BLK, D), BF16),
            V((BLK, D), BF16),
            V((128, D), BF16),
            V((128, D), BF16),
            pltpu.SemaphoreType.DMA((N_SEND,)),
            pltpu.SemaphoreType.DMA((N_RECV,)),
            pltpu.SemaphoreType.DMA((16,)),
        ],
        compiler_params=pltpu.CompilerParams(
            collective_id=0,
            has_side_effects=True,
            vmem_limit_bytes=67_000_000,
        ),
        cost_estimate=pl.CostEstimate(
            flops=20_000_000_000, bytes_accessed=10_000_000, transcendentals=4_000_000
        ),
    )(
        queries,
        keys.T,
        values.T,
        drow,
        sinks,
        residual,
        out_weight,
        norm_gain.reshape(1, D),
        w_gate,
        w_value,
        conv_gate,
        conv_value,
        wdt,
    )


def solution(mesh):
    return jax.shard_map(
        per_device,
        mesh=mesh,
        in_specs=(
            P("sp", "tp"),
            P("sp", "tp"),
            P("sp", "tp"),
            P("sp"),
            P("tp"),
            P(("sp", "tp"), None),
            P("tp", None),
            P(),
            P("sp", "tp"),
            P("sp", "tp"),
            P(None, "tp"),
            P(None, "tp"),
            P("tp", "sp"),
        ),
        out_specs=P(("sp", "tp"), None),
        check_vma=False,
    )
```

```python
import functools

import jax
import jax.numpy as jnp
from jax import lax
from jax.experimental import pallas as pl
from jax.experimental.pallas import tpu as pltpu
from jax.sharding import PartitionSpec as P

HEAD_DIM = 64
WINDOW = 128
MESH = pl.DeviceIdType.MESH
F32 = jnp.float32
BF16 = jnp.bfloat16
NT = (((1,), (1,)), ((), ()))

N_SP = 32
ROWS = 1024
BLK = 256
D = 2048
HID = 1408
HALO = 8
HALF = BLK // 2
EXT = HALF + HALO
PAIR = 2 * EXT
N_SEND, N_RECV = 40, 64
R1, L0, R0, L1, O0, O1, A0, A1 = range(8)
FIRST = {0: O0, 1: R0, 2: A0, 3: L0}
POS = {0: 0, 1: 1, 3: 2, 2: 3}
TN = (((0,), (0,)), ((), ()))


def ceil_dot(a, b):
    return jnp.dot(a, b, preferred_element_type=F32)


def nt_dot(a, b):
    return lax.dot_general(a, b, NT, preferred_element_type=F32)


def kernel(
    q_in,
    k_in,
    v_in,
    drow_in,
    sinks,
    res_in,
    ow_in,
    gain_in,
    wg_in,
    wv_in,
    cg_in,
    cv_in,
    wd_in,
    out,
    q,
    kvt,
    kvz,
    drow,
    dcol,
    m1,
    m2,
    att,
    af,
    via,
    ow,
    res,
    mid,
    gain,
    nb,
    wu,
    wd,
    pre,
    pre0,
    hid,
    cg,
    cv,
    s1,
    s2,
    s3,
    p3,
    rl,
    rr,
    tl,
    tr,
    send_sem,
    recv_sem,
    loc_sem,
):
    sp = lax.axis_index("sp")
    x = lax.axis_index("tp")
    c = lax.rem(sp, 2)
    k = lax.div(sp, 2)
    y = lax.rem(k, 4)
    z = lax.div(k, 4)

    def sp_of(zz, yy):
        return (lax.rem(zz + 8, 4) * 4 + lax.rem(yy + 8, 4)) * 2 + c

    def xat(j):
        return lax.rem(x + j + 4, 4)

    def dev(s, t):
        return {"sp": s, "tp": t}

    sp_next = lax.rem(sp + 1, N_SP)
    sp_prev = lax.rem(sp + N_SP - 1, N_SP)
    sib = sp + 1 - 2 * c
    right, left = dev(sp, xat(1)), dev(sp, xat(3))

    scopes = []

    def phase(name):
        if scopes:
            scopes.pop().__exit__(None, None, None)
        if name:
            scopes.append(jax.named_scope(name))
            scopes[-1].__enter__()

    phase("local")
    bar = pltpu.get_barrier_semaphore()

    def hello(d):
        pl.semaphore_signal(bar, inc=1, device_id=d, device_id_type=MESH)

    for j in (1, 2, 3):
        hello(dev(sp, xat(j)))
    for dz, dy in ((0, 1), (0, -1), (1, 0), (-1, 0)):
        hello(dev(sp_of(z + dz, y + dy), x))
    hello(dev(sib, x))
    for j in range(4):
        hello(dev(sp_prev, xat(j)))

    loc = []

    def local(src, dst):
        cp = pltpu.make_async_copy(src, dst, loc_sem.at[len(loc)])
        cp.start()
        loc.append(cp)
        return cp

    l_k = local(k_in, kvt.at[pl.ds(0, 64), pl.ds(WINDOW, ROWS)])
    l_v = local(v_in, kvt.at[pl.ds(64, 64), pl.ds(WINDOW, ROWS)])
    l_drow = local(drow_in, drow.at[pl.ds(8, 8)])
    l_ow = local(ow_in, ow.at[0])
    row64 = pl.ds(pl.multiple_of(sp * 64, 64), 64)
    l_wg = local(wg_in, wu.at[row64, pl.ds(0, HID)])
    l_wv = local(wv_in, wu.at[row64, pl.ds(HID, HID)])
    l_q = local(q_in, q)
    l_wd = local(wd_in, wd.at[row64])
    l_res = local(res_in, res)
    l_gain = local(gain_in, gain)
    l_cg = local(cg_in, cg)
    l_cv = local(cv_in, cv)

    er = lax.broadcasted_iota(jnp.int32, (128, 2048), 0)
    ec = lax.broadcasted_iota(jnp.int32, (128, 2048), 1)
    sel = (
        ((er >> 6) == (ec >> 10))
        & ((er & 63) == (ec & 63))
        & (((ec >> 8) & 3) == ((ec >> 6) & 3))
    )
    place = jnp.where(sel, 1.0, 0.0).astype(BF16)

    def column(i, _):
        r = pl.ds(pl.multiple_of(HALO + i * 128, 8), 128)
        dcol[r, :] = jnp.broadcast_to(drow[pl.ds(8 + i, 1), :].astype(F32), (128, 128)).T
        return 0

    l_drow.wait()
    lax.fori_loop(0, 8, column, 0)

    phase("barrier")
    pl.semaphore_wait(bar, 12)

    phase("send0")
    copies = []
    used = {"s": 0, "r": 0}

    def new(kind):
        used[kind] += 1
        return (send_sem if kind == "s" else recv_sem).at[used[kind] - 1]

    def push(src, dst, d, ss=None, rs=None):
        cp = pltpu.make_async_remote_copy(
            src_ref=src,
            dst_ref=dst,
            send_sem=new("s") if ss is None else ss,
            recv_sem=new("r") if rs is None else rs,
            device_id=d,
            device_id_type=MESH,
        )
        cp.start()
        if ss is None:
            copies.append(cp)
        return cp

    def wait_all(sem, view):
        pltpu.make_async_copy(view, view, sem).wait()

    l_k.wait()
    l_v.wait()
    nxt = dev(sp_next, x)
    first = sp == 0
    last = sp == N_SP - 1

    def remote(src, dst, d):
        return pltpu.make_async_remote_copy(
            src_ref=src,
            dst_ref=dst,
            send_sem=new("s"),
            recv_sem=new("r"),
            device_id=d,
            device_id_type=MESH,
        )

    h_kv = remote(kvt.at[:, pl.ds(ROWS, WINDOW)], kvt.at[:, pl.ds(0, WINDOW)], nxt)
    h_drow = remote(drow.at[pl.ds(8, 8)], drow.at[pl.ds(0, 8)], nxt)

    @pl.when(jnp.logical_not(last))
    def _():
        h_kv.start()
        h_drow.start()

    @pl.when(first)
    def _():
        kvt[:, 0:WINDOW] = jnp.zeros((128, WINDOW), BF16)
        drow[0:8, :] = jnp.zeros((8, 128), jnp.int32)

    def wu_view(half, kk, cc, part):
        r = (kk * 2 + cc) * 64
        n = 64 if part is None else 32
        if part == 1:
            r = r + 32
        return wu.at[pl.ds(pl.multiple_of(r, 32), n), pl.ds(half * HID, HID)]

    def wd_view(half, kk, cc, part):
        r = (kk * 2 + cc) * 64 + 32 * half
        n = 32 if part is None else 16
        if part == 1:
            r = r + 16
        return wd.at[pl.ds(pl.multiple_of(r, 16), n)]

    def yz(half, n):
        dy, dz = (n, 0) if half == 0 else (0, n)
        return dev(sp_of(z + dz, y + dy), x)

    class Group:
        def __init__(self, size):
            self.size = size
            self.ss = new("s")
            self.sent = 0
            self.sem = {}
            self.due = {}

        def go(self, key, ref, units, d, dst=None):
            if key not in self.sem:
                self.sem[key] = new("r")
                self.due[key] = 0
            push(ref, ref if dst is None else dst, d, self.ss, self.sem[key])
            self.due[key] += units
            self.sent += units

        def come(self, key):
            wait_all(self.sem[key], self.size(self.due[key]))

        def share(self, ref, units=2, key="sib"):
            self.go(key, ref, units, dev(sib, x))

        def s5(self):
            self.come("sib")

        def gone(self):
            wait_all(self.ss, self.size(self.sent))

    class Gather(Group):
        def __init__(self, view, size):
            super().__init__(size)
            self.view = view

        def at(self, half, dp, dq, part=None):
            dy, dz = (dp, dq) if half == 0 else (dq, dp)
            kk = lax.rem(z + dz + 8, 4) * 4 + lax.rem(y + dy + 8, 4)
            return self.view(half, kk, c, part)

        def p(self, half, n):
            return yz(half, n)

        def q(self, half, n):
            return yz(1 - half, n)

        def s0p(self):
            for half in (0, 1):
                b = self.at(half, 0, 0)
                self.go("p", b, 2, self.p(half, 1))
                self.go("p", b, 2, self.p(half, -1))

        def s1p(self):
            self.come("p")
            for half in (0, 1):
                self.go("pf", self.at(half, -1, 0, 0), 1, self.p(half, 1))
                self.go("pf", self.at(half, 1, 0, 1), 1, self.p(half, -1))

        def s1q(self, dp):
            for half in (0, 1):
                b = self.at(half, dp, 0)
                self.go(("q", dp), b, 2, self.q(half, 1))
                self.go(("q", dp), b, 2, self.q(half, -1))
                self.share(b)

        def s2(self):
            self.come("pf")
            self.s1q(2)

        def s3(self, dps):
            for dp in dps:
                self.come(("q", dp))
                for half in (0, 1):
                    lo, hi = self.at(half, dp, -1), self.at(half, dp, 1)
                    if dp in (0, 1):
                        self.go(("f", dp), lo, 2, self.q(half, 1))
                    else:
                        self.go(("f", dp), hi, 2, self.q(half, -1))
                    self.share(lo)
                    self.share(hi)

        def s4(self, dps):
            for dp in dps:
                self.come(("f", dp))
                for half in (0, 1):
                    self.share(self.at(half, dp, 2))

    class GatherOut(Group):
        def at(self, j, par, r, n):
            r = lax.rem(y + z + par, 2) * 128 + r
            cols = pl.ds(pl.multiple_of(c * 1024, 1024), 1024)
            return ow.at[POS[j % 4], pl.ds(pl.multiple_of(r, 32), n), cols]

        def piece(self, j, half):
            return self.at(j, 0, half * 64, 64)

        def over(self, key, j, half, to):
            d = right if to == 1 else left
            self.go(key, self.piece(j, half), 4, d, self.piece(j - to, half))

        def spread(self, j, half, n):
            for i in (0, 1):
                self.go(("y", n), self.at(j, 0, half * 64 + i * 32, 32), 2, yz(half, 1 - 2 * i))
            self.share(self.piece(j, half), 4, ("sib", n == 2))

        def s0(self):
            self.over("x0", 0, 0, 1)
            self.over("x0", 0, 1, -1)
            self.over("x1", 0, 1, 1)
            self.over("x1", 0, 0, -1)

        def s1a(self):
            self.come("x0")
            self.over("xf", 3, 0, 1)
            self.over("xf", 1, 1, -1)
            self.spread(3, 0, 0)
            self.spread(1, 1, 0)

        def s1b(self):
            self.come("x1")
            self.spread(3, 1, 1)
            self.spread(1, 0, 1)

        def s2(self):
            self.come("xf")
            self.spread(2, 0, 2)
            self.spread(2, 1, 2)

        def s4(self, n):
            self.come(("y", n))
            for j, half in (((3, 0), (1, 1)), ((3, 1), (1, 0)), ((2, 0), (2, 1)))[n]:
                self.share(self.at(j, 1, half * 64, 64), 4, ("sib", n == 2))

    def ow_size(n):
        for quarters in (1, 2, 3, 4):
            if n * 8 % quarters == 0 and n * 8 // quarters <= 256:
                return ow.at[pl.ds(0, quarters), pl.ds(0, n * 8 // quarters)]

    g_o = GatherOut(ow_size)
    g_u = Gather(wu_view, lambda n: wu.at[pl.ds(0, 16 * n)])
    g_d = Gather(wd_view, lambda n: wd.at[pl.ds(0, 16 * n)])

    l_ow.wait()
    g_o.s0()
    l_wg.wait()
    l_wv.wait()
    g_u.s0p()

    phase("expand")

    def expand(i, _):
        r = pl.ds(pl.multiple_of(i * 128, 128), 128)
        kvz[r, :] = lax.dot_general(kvt[:, r], place, TN, preferred_element_type=F32).astype(BF16)
        return 0

    lax.fori_loop(1, 9, expand, 0)
    phase("wait_halo")

    @pl.when(jnp.logical_not(first))
    def _():
        h_kv.wait_recv()
        h_drow.wait_recv()

    phase("masks")
    expand(0, 0)
    ahead = jnp.broadcast_to(drow[7:8, :].astype(F32), (128, 128)).T
    dcol[0:HALO, :] = ahead[128 - HALO :, :]

    t_ids = lax.broadcasted_iota(jnp.int32, (ROWS, 128), 0)
    center = dcol[HALO : HALO + ROWS, :]
    ok1 = (dcol[HALO - 1 : HALO - 1 + ROWS, :] == center) & ((t_ids >= 1) | jnp.logical_not(first))
    ok2 = (dcol[HALO - 2 : HALO - 2 + ROWS, :] == center) & ((t_ids >= 2) | jnp.logical_not(first))
    m1[...] = jnp.where(ok1, 1.0, 0.0)
    m2[...] = jnp.where(ok2, 1.0, 0.0)

    l_q.wait()

    ri = lax.broadcasted_iota(jnp.int32, (128, 128), 0)
    ci = lax.broadcasted_iota(jnp.int32, (128, 128), 1)

    def attend(b):
        r0 = pl.multiple_of(b * 128, 128)
        qb = q[pl.ds(r0, 128), :]
        keys = pl.ds(r0, 256)
        dq = dcol[pl.ds(pl.multiple_of(HALO + b * 128, 8), 128), :]
        k0 = drow[pl.ds(7 + b, 1), :].astype(F32)
        k1 = drow[pl.ds(8 + b, 1), :].astype(F32)
        there = jnp.logical_not(first & (b == 0))
        lower = (dq == k0) & (ci > ri) & there
        upper = (dq == k1) & (ci <= ri)
        keep = jnp.concatenate([lower, upper], axis=1)
        o = jnp.zeros((128, 256), F32)
        for h in range(4):
            s = nt_dot(qb, kvz[keys, h * 256 : (h + 1) * 256]) * (HEAD_DIM**-0.5)
            s = jnp.where(keep, s, -jnp.inf)
            sink = sinks[h]
            peak = jnp.maximum(jnp.max(s, axis=-1, keepdims=True), sink)
            e = jnp.exp(s - peak)
            total = jnp.sum(e, axis=-1, keepdims=True) + jnp.exp(sink - peak)
            p = (e / total).astype(BF16)
            o = o + ceil_dot(p, kvz[keys, 1024 + h * 256 : 1024 + (h + 1) * 256])
        att[pl.ds(r0, 128), :] = o.astype(BF16)

    a2a, over, across = {}, [], []

    def af_col(j):
        return af.at[:, pl.ds(POS[(-j) % 4] * 256, 256)]

    for j in (2, 1, 3, 0):
        t = xat(j)

        def two(i, _, t=t):
            attend(t * 2 + i)
            return 0

        phase(f"attend{j}")
        lax.fori_loop(0, 2, two, 0)
        rows = att.at[pl.ds(pl.multiple_of(t * 256, 256), 256)]
        if j == 2:
            for h, d in ((0, right), (1, left)):
                half = att.at[pl.ds(pl.multiple_of(t * 256 + h * 128, 128), 128)]
                over.append(push(half, via.at[h], d))
        elif j:
            a2a[j] = push(rows, af_col(j), dev(sp, t))
        else:
            l_af = local(rows, af_col(0))
        if j == 2:
            phase("o1a")
            g_o.s1a()
            phase("d0p")
            l_wd.wait()
            g_d.s0p()
        if j == 1:
            phase("o1b")
            g_o.s1b()
        if j == 3:
            phase("a2f")
            for h, d in ((0, right), (1, left)):
                over[h].wait_recv()
                across.append(push(via.at[h], af_col(2).at[pl.ds(h * 128, 128)], d))
            phase("u1p")
            g_u.s1p()
    phase("o2")
    g_o.s2()
    phase("u1")
    g_u.s1q(0)
    g_u.s1q(-1)
    g_u.s1q(1)
    g_o.s4(0)
    phase("a2a")
    l_af.wait()
    for cp in (a2a[1], a2a[3], *across):
        cp.wait_recv()
    phase("o4")
    g_o.s4(1)
    l_res.wait()
    l_gain.wait()
    l_cg.wait()
    l_cv.wait()
    phase("o5a")
    g_o.come(("sib", False))

    phase("project1")

    def project1(j, _):
        col = pl.ds(pl.multiple_of(j * 512, 512), 512)
        w = ow[0:3, :, col].reshape(768, 512)
        mid[:, col] = res[:, col].astype(F32) + ceil_dot(af[:, 0:768], w)
        return 0

    lax.fori_loop(0, D // 512, project1, 0)
    phase("o4b")
    g_o.s4(2)
    phase("u2")
    g_u.s2()
    phase("o5b")
    g_o.come(("sib", True))
    phase("project2")

    def project2(j, sq):
        col = pl.ds(pl.multiple_of(j * 512, 512), 512)
        m = mid[:, col] + ceil_dot(af[:, 768:1024], ow[3, :, col])
        m = m.astype(BF16).astype(F32)
        mid[:, col] = m
        return sq + jnp.sum(m * m, axis=-1, keepdims=True)

    sq = lax.fori_loop(0, D // 512, project2, jnp.zeros((BLK, 1), F32))
    inv = lax.rsqrt(sq * (1.0 / D) + 1e-06)
    for h in (0, 1):
        r = slice(h * HALF, (h + 1) * HALF)
        for j in range(D // 512):
            col = slice(j * 512, (j + 1) * 512)
            n = (mid[r, col] * inv[r] * gain[:, col]).astype(BF16)
            nb[O0 + h, HALO:EXT, col] = n
            if h == 0:
                nb[O1, 0:HALO, col] = n[HALF - HALO :]

    phase("send_n")

    def rows_of(i):
        return nb.at[i, pl.ds(HALO, HALF)]

    def halo_of(i):
        return nb.at[i, pl.ds(0, HALO)]

    tail = nb.at[O1, pl.ds(HALF, HALO)]
    t_sp = jnp.where(x == 3, sp_next, sp)
    n_mid = push(halo_of(O1), halo_of(R1), left)
    tails = [push(tail, halo_of(FIRST[(1 - j) % 4]), dev(t_sp, xat(j))) for j in (1, 3)]
    n_r0 = push(rows_of(O0), rows_of(L0), right)
    n_l1 = push(rows_of(O1), rows_of(R1), left)
    tails.append(push(tail, halo_of(FIRST[3]), dev(t_sp, xat(2))))
    tail0 = pltpu.make_async_remote_copy(
        src_ref=tail,
        dst_ref=halo_of(R0),
        send_sem=new("s"),
        recv_sem=new("r"),
        device_id=dev(sp_next, x),
        device_id_type=MESH,
    )
    tail0_local = pltpu.make_async_copy(tail, halo_of(R0), loc_sem.at[len(loc)])
    loc.append(None)

    @pl.when(x == 3)
    def _():
        tail0.start()

    @pl.when(x != 3)
    def _():
        tail0_local.start()

    n_r1 = push(rows_of(O1), rows_of(L1), right)
    n_l0 = push(rows_of(O0), rows_of(R0), left)

    phase("u3a")
    g_u.s3((0,))
    g_d.s1p()
    phase("u3b")
    g_u.s3((-1,))
    phase("u3c")
    g_u.s3((1,))
    g_d.s1q(0)
    phase("u3d")
    g_u.s3((2,))
    g_d.s1q(-1)
    g_d.s1q(1)
    phase("d2")
    g_d.s2()
    phase("u4a")
    g_u.s4((0, -1))
    phase("n_half")
    n_r0.wait_recv()
    f_r = push(rows_of(L0), rows_of(A0), right)
    n_l1.wait_recv()
    f_l = push(rows_of(R1), rows_of(A1), left)
    phase("u4c")
    g_u.s4((1, 2))
    phase("d3a")
    g_d.s3((0,))
    phase("u5")
    g_u.s5()
    phase("tails")
    n_mid.wait_recv()
    for cp in tails:
        cp.wait_recv()

    @pl.when(x == 3)
    def _():
        tail0.wait()

    @pl.when(x != 3)
    def _():
        tail0_local.wait()

    def up(i, to, parts=(0, 1)):
        rows = nb[i : i + 2].reshape(PAIR, D)
        for h in parts:
            col = pl.ds(h * HID, HID)
            to[:, col] = ceil_dot(rows, wu[:, col]).astype(BF16).astype(F32)

    def conv(i, pre, blocks):
        def step(j, _):
            gc = pl.ds(pl.multiple_of(j * 128, 128), 128)
            vc = pl.ds(pl.multiple_of(HID + j * 128, 128), 128)
            tg = cg[:, gc]
            tv = cv[:, gc]
            for n, (d, h) in enumerate(blocks):
                for r in range(0, HALF, 64):
                    mr = pl.ds(pl.multiple_of(d * BLK + h * HALF + r, 64), 64)
                    k1 = m1[mr, :] > 0.5
                    k2 = m2[mr, :] > 0.5
                    r0 = n * EXT + HALO + r

                    def taps(t, cc):
                        a = t[2:3] * pre[r0 : r0 + 64, cc]
                        a = a + jnp.where(k1, t[1:2] * pre[r0 - 1 : r0 + 63, cc], 0.0)
                        return a + jnp.where(k2, t[0:1] * pre[r0 - 2 : r0 + 62, cc], 0.0)

                    g = taps(tg, gc)
                    v = taps(tv, vc)
                    o = n * HALF + r
                    hid[i // 2, o : o + 64, gc] = (g / (1.0 + jnp.exp(-g)) * v).astype(BF16)
            return 0

        lax.fori_loop(0, HID // 128, step, 0)

    chunks = (pl.ds(0, 1024), pl.ds(1024, 1024))
    top, bot = pl.ds(0, HALF), pl.ds(HALF, HALF)

    def down(i, col):
        return nt_dot(hid[i // 2], wd[col, :])

    phase("up1")
    up(R1, pre)
    phase("d3b")
    g_d.s3((-1, 1))
    phase("d3c")
    g_d.s3((2,))
    g_d.s4((0,))
    phase("conv1")
    conv(R1, pre, ((xat(1), 1), (xat(3), 0)))
    phase("up0a")
    up(O0, pre0, (0,))
    phase("d4a")
    g_d.s4((-1, 1))
    phase("up0b")
    up(O0, pre0, (1,))
    phase("d4b")
    g_d.s4((2,))
    phase("d5")
    g_d.s5()
    phase("down1")
    s_one, s_two, s_three = [], [], []
    for col in chunks:
        a = down(R1, col)
        s1[:, col] = a.astype(BF16)
        s_one.append(push(s1.at[top, col], rl.at[bot, col], right))
        s_one.append(push(s1.at[bot, col], rr.at[top, col], left))

    phase("conv0")
    conv(O0, pre0, ((x, 0), (x, 1)))

    phase("wait_n2")
    f_r.wait_recv()
    f_l.wait_recv()
    nb[A1, 0:HALO, :] = nb[A0, HALF:EXT, :]
    phase("up2")
    up(A0, pre)
    phase("conv2")
    conv(A0, pre, ((xat(2), 0), (xat(2), 1)))
    phase("down2")
    for col in chunks:
        s2[:, col] = down(A0, col).astype(BF16)
        s_two.append(
            (
                push(s2.at[top, col], tl.at[:, col], right),
                push(s2.at[bot, col], tr.at[:, col], left),
            )
        )

    phase("wait_n1")
    n_l0.wait_recv()
    n_r1.wait_recv()
    nb[L1, 0:HALO, :] = nb[L0, HALF:EXT, :]
    phase("up3")
    up(R0, pre)
    phase("conv3")
    conv(R0, pre, ((xat(1), 0), (xat(3), 1)))
    phase("down3")
    for col in chunks:
        p3[:, col] = down(R0, col)

    def finish(i, col):
        s_two[i][0].wait_recv()
        s3[top, col] = (p3[top, col] + tl[:, col].astype(F32)).astype(BF16)
        s_three.append(push(s3.at[top, col], rl.at[top, col], right))
        s_two[i][1].wait_recv()
        s3[bot, col] = (p3[bot, col] + tr[:, col].astype(F32)).astype(BF16)
        s_three.append(push(s3.at[bot, col], rr.at[bot, col], left))

    phase("down0")
    for col in chunks:
        mid[:, col] += down(O0, col)
    for i, col in enumerate(chunks):
        phase("wait_t")
        finish(i, col)

    phase("wait_s1")
    for cp in s_one:
        cp.wait_recv()
    for i, col in enumerate(chunks):
        phase("wait_s3")
        s_three[2 * i].wait_recv()
        s_three[2 * i + 1].wait_recv()
        phase("final")
        out[:, col] = (mid[:, col] + rl[:, col].astype(F32) + rr[:, col].astype(F32)).astype(BF16)
    phase("wait_sends")
    for cp in copies:
        cp.wait_send()

    @pl.when(jnp.logical_not(last))
    def _():
        h_kv.wait_send()
        h_drow.wait_send()

    for g in (g_o, g_u, g_d):
        g.gone()
    phase(None)
    assert used["s"] <= N_SEND and used["r"] <= N_RECV, used


def per_device(
    queries,
    keys,
    values,
    doc_ids,
    sinks,
    residual,
    out_weight,
    norm_gain,
    w_gate,
    w_value,
    conv_gate,
    conv_value,
    w_down,
):
    drow = doc_ids.reshape(8, 128)
    wdt = w_down.T
    any_spec = pl.BlockSpec(memory_space=pl.ANY)
    smem = pl.BlockSpec(memory_space=pltpu.SMEM)
    V = pltpu.VMEM
    i32 = jnp.int32
    return pl.pallas_call(
        kernel,
        out_shape=pltpu.VMEM((BLK, D), BF16),
        in_specs=[any_spec] * 4 + [smem] + [any_spec] * 8,
        out_specs=pl.BlockSpec(memory_space=pltpu.VMEM),
        scratch_shapes=[
            V((ROWS, 256), BF16),
            V((128, ROWS + WINDOW), BF16),
            V((ROWS + WINDOW, 2048), BF16),
            V((16, 128), i32),
            V((ROWS + HALO, 128), F32),
            V((ROWS, 128), F32),
            V((ROWS, 128), F32),
            V((ROWS, 256), BF16),
            V((BLK, 1024), BF16),
            V((2, HALF, 256), BF16),
            V((4, 256, D), BF16),
            V((BLK, D), BF16),
            V((BLK, D), F32),
            V((1, D), F32),
            V((8, EXT, D), BF16),
            V((D, 2 * HID), BF16),
            V((D, HID), BF16),
            V((PAIR, 2 * HID), F32),
            V((PAIR, 2 * HID), F32),
            V((4, BLK, HID), BF16),
            V((3, HID), F32),
            V((3, HID), F32),
            V((BLK, D), BF16),
            V((BLK, D), BF16),
            V((BLK, D), BF16),
            V((BLK, D), F32),
            V((BLK, D), BF16),
            V((BLK, D), BF16),
            V((128, D), BF16),
            V((128, D), BF16),
            pltpu.SemaphoreType.DMA((N_SEND,)),
            pltpu.SemaphoreType.DMA((N_RECV,)),
            pltpu.SemaphoreType.DMA((16,)),
        ],
        compiler_params=pltpu.CompilerParams(
            collective_id=0,
            has_side_effects=True,
            vmem_limit_bytes=62_000_000,
        ),
        cost_estimate=pl.CostEstimate(
            flops=20_000_000_000, bytes_accessed=10_000_000, transcendentals=4_000_000
        ),
    )(
        queries,
        keys.T,
        values.T,
        drow,
        sinks,
        residual,
        out_weight,
        norm_gain.reshape(1, D),
        w_gate,
        w_value,
        conv_gate,
        conv_value,
        wdt,
    )


def solution(mesh):
    return jax.shard_map(
        per_device,
        mesh=mesh,
        in_specs=(
            P("sp", "tp"),
            P("sp", "tp"),
            P("sp", "tp"),
            P("sp"),
            P("tp"),
            P(("sp", "tp"), None),
            P("tp", None),
            P(),
            P("sp", "tp"),
            P("sp", "tp"),
            P(None, "tp"),
            P(None, "tp"),
            P("tp", "sp"),
        ),
        out_specs=P(("sp", "tp"), None),
        check_vma=False,
    )
```

```python
import functools

import jax
import jax.numpy as jnp
from jax import lax
from jax.experimental import pallas as pl
from jax.experimental.pallas import tpu as pltpu
from jax.sharding import PartitionSpec as P

HEAD_DIM = 64
WINDOW = 128
MESH = pl.DeviceIdType.MESH
F32 = jnp.float32
BF16 = jnp.bfloat16
NT = (((1,), (1,)), ((), ()))

N_SP = 32
ROWS = 1024
BLK = 256
D = 2048
HID = 1408
HALO = 8
HALF = BLK // 2
EXT = HALF + HALO
PAIR = 2 * EXT
N_SEND, N_RECV = 40, 64
R1, L0, R0, L1, O0, O1, A0, A1 = range(8)
POS = {0: 0, 1: 1, 3: 2, 2: 3}
TN = (((0,), (0,)), ((), ()))


def ceil_dot(a, b):
    return jnp.dot(a, b, preferred_element_type=F32)


def nt_dot(a, b):
    return lax.dot_general(a, b, NT, preferred_element_type=F32)


def kernel(
    q_in,
    k_in,
    v_in,
    drow_in,
    sinks,
    res_in,
    ow_in,
    gain_in,
    wg_in,
    wv_in,
    cg_in,
    cv_in,
    wd_in,
    out,
    q,
    kvt,
    kvz,
    drow,
    dcol,
    m1,
    m2,
    att,
    af,
    via,
    ow,
    res,
    mid,
    gain,
    nb,
    edge,
    wu,
    wd,
    pre,
    pre0,
    hid,
    cg,
    cv,
    s1,
    s2,
    s3,
    p3,
    rl,
    rr,
    tl,
    tr,
    send_sem,
    recv_sem,
    loc_sem,
):
    sp = lax.axis_index("sp")
    x = lax.axis_index("tp")
    c = lax.rem(sp, 2)
    k = lax.div(sp, 2)
    y = lax.rem(k, 4)
    z = lax.div(k, 4)

    def sp_of(zz, yy):
        return (lax.rem(zz + 8, 4) * 4 + lax.rem(yy + 8, 4)) * 2 + c

    def xat(j):
        return lax.rem(x + j + 4, 4)

    def dev(s, t):
        return {"sp": s, "tp": t}

    sp_next = lax.rem(sp + 1, N_SP)
    sp_prev = lax.rem(sp + N_SP - 1, N_SP)
    sib = sp + 1 - 2 * c
    right, left = dev(sp, xat(1)), dev(sp, xat(3))

    scopes = []

    def phase(name):
        if scopes:
            scopes.pop().__exit__(None, None, None)
        if name:
            scopes.append(jax.named_scope(name))
            scopes[-1].__enter__()

    phase("local")
    bar = pltpu.get_barrier_semaphore()

    def hello(d):
        pl.semaphore_signal(bar, inc=1, device_id=d, device_id_type=MESH)

    for j in (1, 2, 3):
        hello(dev(sp, xat(j)))
    for dz, dy in ((0, 1), (0, -1), (1, 0), (-1, 0)):
        hello(dev(sp_of(z + dz, y + dy), x))
    hello(dev(sib, x))
    for j in range(4):
        hello(dev(sp_prev, xat(j)))

    loc = []

    def local(src, dst):
        cp = pltpu.make_async_copy(src, dst, loc_sem.at[len(loc)])
        cp.start()
        loc.append(cp)
        return cp

    l_k = local(k_in, kvt.at[pl.ds(0, 64), pl.ds(WINDOW, ROWS)])
    l_v = local(v_in, kvt.at[pl.ds(64, 64), pl.ds(WINDOW, ROWS)])
    l_drow = local(drow_in, drow.at[pl.ds(8, 8)])
    l_ow = local(ow_in, ow.at[0])
    row64 = pl.ds(pl.multiple_of(sp * 64, 64), 64)
    l_wg = local(wg_in, wu.at[row64, pl.ds(0, HID)])
    l_wv = local(wv_in, wu.at[row64, pl.ds(HID, HID)])
    l_q = local(q_in, q)
    l_wd = local(wd_in, wd.at[row64])
    l_res = local(res_in, res)
    l_gain = local(gain_in, gain)
    l_cg = local(cg_in, cg)
    l_cv = local(cv_in, cv)

    phase("barrier")
    pl.semaphore_wait(bar, 12)

    phase("send0")
    copies = []
    used = {"s": 0, "r": 0}

    def new(kind):
        used[kind] += 1
        return (send_sem if kind == "s" else recv_sem).at[used[kind] - 1]

    def push(src, dst, d, ss=None, rs=None):
        cp = pltpu.make_async_remote_copy(
            src_ref=src,
            dst_ref=dst,
            send_sem=new("s") if ss is None else ss,
            recv_sem=new("r") if rs is None else rs,
            device_id=d,
            device_id_type=MESH,
        )
        cp.start()
        if ss is None:
            copies.append(cp)
        return cp

    def wait_all(sem, view):
        pltpu.make_async_copy(view, view, sem).wait()

    l_k.wait()
    l_v.wait()
    l_drow.wait()
    nxt = dev(sp_next, x)
    first = sp == 0
    last = sp == N_SP - 1

    def remote(src, dst, d):
        return pltpu.make_async_remote_copy(
            src_ref=src,
            dst_ref=dst,
            send_sem=new("s"),
            recv_sem=new("r"),
            device_id=d,
            device_id_type=MESH,
        )

    h_kv = remote(kvt.at[:, pl.ds(ROWS, WINDOW)], kvt.at[:, pl.ds(0, WINDOW)], nxt)
    h_drow = remote(drow.at[pl.ds(8, 8)], drow.at[pl.ds(0, 8)], nxt)

    @pl.when(jnp.logical_not(last))
    def _():
        h_kv.start()
        h_drow.start()

    @pl.when(first)
    def _():
        kvt[:, 0:WINDOW] = jnp.zeros((128, WINDOW), BF16)
        drow[0:8, :] = jnp.zeros((8, 128), jnp.int32)

    def wu_view(half, kk, cc, part):
        r = (kk * 2 + cc) * 64
        n = 64 if part is None else 32
        if part == 1:
            r = r + 32
        return wu.at[pl.ds(pl.multiple_of(r, 32), n), pl.ds(half * HID, HID)]

    def wd_view(half, kk, cc, part):
        r = (kk * 2 + cc) * 64 + 32 * half
        n = 32 if part is None else 16
        if part == 1:
            r = r + 16
        return wd.at[pl.ds(pl.multiple_of(r, 16), n)]

    def yz(half, n):
        dy, dz = (n, 0) if half == 0 else (0, n)
        return dev(sp_of(z + dz, y + dy), x)

    class Group:
        def __init__(self, size):
            self.size = size
            self.ss = new("s")
            self.sent = 0
            self.sem = {}
            self.due = {}

        def go(self, key, ref, units, d, dst=None):
            if key not in self.sem:
                self.sem[key] = new("r")
                self.due[key] = 0
            push(ref, ref if dst is None else dst, d, self.ss, self.sem[key])
            self.due[key] += units
            self.sent += units

        def come(self, key):
            wait_all(self.sem[key], self.size(self.due[key]))

        def share(self, ref, units=2, key="sib"):
            self.go(key, ref, units, dev(sib, x))

        def s5(self):
            self.come("sib")

        def gone(self):
            wait_all(self.ss, self.size(self.sent))

    class Gather(Group):
        def __init__(self, view, size):
            super().__init__(size)
            self.view = view

        def at(self, half, dp, dq, part=None):
            dy, dz = (dp, dq) if half == 0 else (dq, dp)
            kk = lax.rem(z + dz + 8, 4) * 4 + lax.rem(y + dy + 8, 4)
            return self.view(half, kk, c, part)

        def p(self, half, n):
            return yz(half, n)

        def q(self, half, n):
            return yz(1 - half, n)

        def s0p(self):
            for half in (0, 1):
                b = self.at(half, 0, 0)
                self.go("p", b, 2, self.p(half, 1))
                self.go("p", b, 2, self.p(half, -1))

        def s1p(self):
            self.come("p")
            for half in (0, 1):
                self.go("pf", self.at(half, -1, 0, 0), 1, self.p(half, 1))
                self.go("pf", self.at(half, 1, 0, 1), 1, self.p(half, -1))

        def s1q(self, dp, part=None):
            n = 2 if part is None else 1
            for half in (0, 1):
                b = self.at(half, dp, 0, part)
                self.go(("q", dp), b, n, self.q(half, 1))
                self.go(("q", dp), b, n, self.q(half, -1))
                self.share(b, n)

        def s2(self):
            self.come("pf")
            self.s1q(2)

        def s3(self, dps):
            for dp in dps:
                self.come(("q", dp))
                for half in (0, 1):
                    lo, hi = self.at(half, dp, -1), self.at(half, dp, 1)
                    if dp in (0, 1):
                        self.go(("f", dp), lo, 2, self.q(half, 1))
                    else:
                        self.go(("f", dp), hi, 2, self.q(half, -1))
                    self.share(lo)
                    self.share(hi)

        def s4(self, dps):
            for dp in dps:
                self.come(("f", dp))
                for half in (0, 1):
                    self.share(self.at(half, dp, 2))

    class GatherOut(Group):
        def at(self, j, par, r, n):
            r = lax.rem(y + z + par, 2) * 128 + r
            cols = pl.ds(pl.multiple_of(c * 1024, 1024), 1024)
            return ow.at[POS[j % 4], pl.ds(pl.multiple_of(r, 32), n), cols]

        def piece(self, j, half):
            return self.at(j, 0, half * 64, 64)

        def over(self, key, j, half, to):
            d = right if to == 1 else left
            self.go(key, self.piece(j, half), 4, d, self.piece(j - to, half))

        def spread(self, j, half, n):
            for i in (0, 1):
                self.go(("y", n), self.at(j, 0, half * 64 + i * 32, 32), 2, yz(half, 1 - 2 * i))
            self.share(self.piece(j, half), 4, ("sib", n == 2))

        def s0(self):
            self.over("x0", 0, 0, 1)
            self.over("x0", 0, 1, -1)
            self.over("x1", 0, 1, 1)
            self.over("x1", 0, 0, -1)

        def s1a(self):
            self.come("x0")
            self.over("xf", 3, 0, 1)
            self.over("xf", 1, 1, -1)
            self.spread(3, 0, 0)
            self.spread(1, 1, 0)

        def s1b(self):
            self.come("x1")
            self.spread(3, 1, 1)
            self.spread(1, 0, 1)

        def s2(self):
            self.come("xf")
            self.spread(2, 0, 2)
            self.spread(2, 1, 2)

        def s4(self, n):
            self.come(("y", n))
            for j, half in (((3, 0), (1, 1)), ((3, 1), (1, 0)), ((2, 0), (2, 1)))[n]:
                self.share(self.at(j, 1, half * 64, 64), 4, ("sib", n == 2))

    def ow_size(n):
        for quarters in (1, 2, 3, 4):
            if n * 8 % quarters == 0 and n * 8 // quarters <= 256:
                return ow.at[pl.ds(0, quarters), pl.ds(0, n * 8 // quarters)]

    g_o = GatherOut(ow_size)
    g_u = Gather(wu_view, lambda n: wu.at[pl.ds(0, 16 * n)])
    g_d = Gather(wd_view, lambda n: wd.at[pl.ds(0, 16 * n)])

    l_ow.wait()
    g_o.s0()
    l_wg.wait()
    l_wv.wait()
    g_u.s0p()

    phase("column")
    er = lax.broadcasted_iota(jnp.int32, (128, 2048), 0)
    ec = lax.broadcasted_iota(jnp.int32, (128, 2048), 1)
    sel = (
        ((er >> 6) == (ec >> 10))
        & ((er & 63) == (ec & 63))
        & (((ec >> 8) & 3) == ((ec >> 6) & 3))
    )
    place = jnp.where(sel, 1.0, 0.0).astype(BF16)

    def column(i, _):
        r = pl.ds(pl.multiple_of(HALO + i * 128, 8), 128)
        dcol[r, :] = jnp.broadcast_to(drow[pl.ds(8 + i, 1), :].astype(F32), (128, 128)).T
        return 0

    lax.fori_loop(0, 8, column, 0)

    phase("expand")

    def expand(i, _):
        r = pl.ds(pl.multiple_of(i * 128, 128), 128)
        kvz[r, :] = lax.dot_general(kvt[:, r], place, TN, preferred_element_type=F32).astype(BF16)
        return 0

    lax.fori_loop(1, 9, expand, 0)
    phase("wait_halo")

    @pl.when(jnp.logical_not(first))
    def _():
        h_kv.wait_recv()
        h_drow.wait_recv()

    phase("masks")
    expand(0, 0)
    ahead = jnp.broadcast_to(drow[7:8, :].astype(F32), (128, 128)).T
    dcol[0:HALO, :] = ahead[128 - HALO :, :]

    t_ids = lax.broadcasted_iota(jnp.int32, (ROWS, 128), 0)
    center = dcol[HALO : HALO + ROWS, :]
    ok1 = (dcol[HALO - 1 : HALO - 1 + ROWS, :] == center) & ((t_ids >= 1) | jnp.logical_not(first))
    ok2 = (dcol[HALO - 2 : HALO - 2 + ROWS, :] == center) & ((t_ids >= 2) | jnp.logical_not(first))
    m1[...] = jnp.where(ok1, 1.0, 0.0)
    m2[...] = jnp.where(ok2, 1.0, 0.0)

    l_q.wait()

    ri = lax.broadcasted_iota(jnp.int32, (128, 128), 0)
    ci = lax.broadcasted_iota(jnp.int32, (128, 128), 1)

    def attend(b):
        r0 = pl.multiple_of(b * 128, 128)
        qb = q[pl.ds(r0, 128), :]
        keys = pl.ds(r0, 256)
        dq = dcol[pl.ds(pl.multiple_of(HALO + b * 128, 8), 128), :]
        k0 = drow[pl.ds(7 + b, 1), :].astype(F32)
        k1 = drow[pl.ds(8 + b, 1), :].astype(F32)
        there = jnp.logical_not(first & (b == 0))
        lower = (dq == k0) & (ci > ri) & there
        upper = (dq == k1) & (ci <= ri)
        keep = jnp.concatenate([lower, upper], axis=1)
        o = jnp.zeros((128, 256), F32)
        for h in range(4):
            s = nt_dot(qb, kvz[keys, h * 256 : (h + 1) * 256]) * (HEAD_DIM**-0.5)
            s = jnp.where(keep, s, -jnp.inf)
            sink = sinks[h]
            peak = jnp.maximum(jnp.max(s, axis=-1, keepdims=True), sink)
            e = jnp.exp(s - peak)
            total = jnp.sum(e, axis=-1, keepdims=True) + jnp.exp(sink - peak)
            p = (e / total).astype(BF16)
            o = o + ceil_dot(p, kvz[keys, 1024 + h * 256 : 1024 + (h + 1) * 256])
        att[pl.ds(r0, 128), :] = o.astype(BF16)

    a2a, over, across = {}, [], []

    def af_col(j):
        return af.at[:, pl.ds(POS[(-j) % 4] * 256, 256)]

    for j in (2, 1, 3, 0):
        t = xat(j)

        def two(i, _, t=t):
            attend(t * 2 + i)
            return 0

        phase(f"attend{j}")
        lax.fori_loop(0, 2, two, 0)
        rows = att.at[pl.ds(pl.multiple_of(t * 256, 256), 256)]
        if j == 2:
            for h, d in ((0, right), (1, left)):
                half = att.at[pl.ds(pl.multiple_of(t * 256 + h * 128, 128), 128)]
                over.append(push(half, via.at[h], d))
        elif j:
            a2a[j] = push(rows, af_col(j), dev(sp, t))
        else:
            l_af = local(rows, af_col(0))
        if j == 2:
            phase("o1a")
            g_o.s1a()
            phase("d0p")
            l_wd.wait()
            g_d.s0p()
        if j == 1:
            phase("o1b")
            g_o.s1b()
        if j == 3:
            phase("a2f")
            for h, d in ((0, right), (1, left)):
                over[h].wait_recv()
                across.append(push(via.at[h], af_col(2).at[pl.ds(h * 128, 128)], d))
            phase("u1p")
            g_u.s1p()
    phase("o2")
    g_o.s2()
    phase("u1")
    g_u.s1q(0)
    g_u.s1q(-1)
    g_u.s1q(1)
    g_o.s4(0)
    phase("o4a")
    g_o.s4(1)
    g_d.s1p()
    phase("a2a")
    l_af.wait()
    for cp in (a2a[1], a2a[3], *across):
        cp.wait_recv()
    l_res.wait()
    l_gain.wait()
    l_cg.wait()
    l_cv.wait()
    phase("o5a")
    g_o.come(("sib", False))

    phase("project1")

    def project1(j, _):
        col = pl.ds(pl.multiple_of(j * 512, 512), 512)
        w = ow[0:3, :, col].reshape(768, 512)
        mid[:, col] = res[:, col].astype(F32) + ceil_dot(af[:, 0:768], w)
        return 0

    lax.fori_loop(0, D // 512, project1, 0)
    phase("o4b")
    g_o.s4(2)
    phase("u2")
    g_u.s2()
    phase("o5b")
    g_o.come(("sib", True))
    phase("project2")

    def project2(j, sq):
        col = pl.ds(pl.multiple_of(j * 512, 512), 512)
        m = mid[:, col] + ceil_dot(af[:, 768:1024], ow[3, :, col])
        m = m.astype(BF16).astype(F32)
        mid[:, col] = m
        return sq + jnp.sum(m * m, axis=-1, keepdims=True)

    sq = lax.fori_loop(0, D // 512, project2, jnp.zeros((BLK, 1), F32))
    inv = lax.rsqrt(sq * (1.0 / D) + 1e-06)
    for h in (0, 1):
        r = slice(h * HALF, (h + 1) * HALF)
        for j in range(D // 512):
            col = slice(j * 512, (j + 1) * 512)
            n = (mid[r, col] * inv[r] * gain[:, col]).astype(BF16)
            nb[O0 + h, HALO:EXT, col] = n
            if h == 0:
                nb[O1, 0:HALO, col] = n[HALF - HALO :]

    phase("send_n")

    def rows_of(i):
        return nb.at[i, pl.ds(HALO, HALF)]

    def halo_of(i):
        return nb.at[i, pl.ds(0, HALO)]

    tail = nb.at[O1, pl.ds(HALF, HALO)]
    n_mid = push(halo_of(O1), halo_of(R1), left)
    n_r0 = push(rows_of(O0), rows_of(L0), right)
    n_l1 = push(rows_of(O1), rows_of(R1), left)
    tails = [push(tail, halo_of(L0), dev(jnp.where(x == 3, sp_next, sp), xat(2)))]
    edges = [remote(tail, edge, dev(sp_next, xat(j))) for j in (0, 1, 3)]
    edge_from = {0: 3, 1: 0, 3: 2}

    @pl.when(x == 3)
    def _():
        for cp in edges:
            cp.start()

    n_r1 = push(rows_of(O1), rows_of(L1), right)
    n_l0 = push(rows_of(O0), rows_of(R0), left)

    phase("u3a")
    g_u.s3((0,))
    phase("u3b")
    g_u.s3((-1,))
    phase("u3c")
    g_u.s3((1,))
    g_d.s1q(0)
    phase("u3d")
    g_u.s3((2,))
    g_d.s1q(-1)
    g_d.s1q(1)
    phase("d2")
    g_d.s2()
    phase("u4a")
    g_u.s4((0, -1))
    phase("n_half")
    n_r0.wait_recv()
    f_r = push(rows_of(L0), rows_of(A0), right)
    n_l1.wait_recv()
    f_l = push(rows_of(R1), rows_of(A1), left)
    phase("u4c")
    g_u.s4((1, 2))
    phase("d3a")
    g_d.s3((0,))
    phase("u5")
    g_u.s5()
    phase("tails")
    n_mid.wait_recv()
    for cp in tails:
        cp.wait_recv()
    for j, cp in zip((0, 1, 3), edges):

        @pl.when(x == edge_from[j])
        def _(cp=cp):
            cp.wait_recv()

    def put_halo(slot, before, edge_x):
        near = nb[before, HALF:EXT, :]
        nb[slot, 0:HALO, :] = jnp.where(x == edge_x, edge[...], near)

    def up(i, to, parts=(0, 1)):
        rows = nb[i : i + 2].reshape(PAIR, D)
        for h in parts:
            col = pl.ds(h * HID, HID)
            to[:, col] = ceil_dot(rows, wu[:, col]).astype(BF16).astype(F32)

    def conv(i, pre, blocks):
        def step(j, _):
            gc = pl.ds(pl.multiple_of(j * 128, 128), 128)
            vc = pl.ds(pl.multiple_of(HID + j * 128, 128), 128)
            tg = cg[:, gc]
            tv = cv[:, gc]
            for n, (d, h) in enumerate(blocks):
                for r in range(0, HALF, 64):
                    mr = pl.ds(pl.multiple_of(d * BLK + h * HALF + r, 64), 64)
                    k1 = m1[mr, :] > 0.5
                    k2 = m2[mr, :] > 0.5
                    r0 = n * EXT + HALO + r

                    def taps(t, cc):
                        a = t[2:3] * pre[r0 : r0 + 64, cc]
                        a = a + jnp.where(k1, t[1:2] * pre[r0 - 1 : r0 + 63, cc], 0.0)
                        return a + jnp.where(k2, t[0:1] * pre[r0 - 2 : r0 + 62, cc], 0.0)

                    g = taps(tg, gc)
                    v = taps(tv, vc)
                    o = n * HALF + r
                    hid[i // 2, o : o + 64, gc] = (g / (1.0 + jnp.exp(-g)) * v).astype(BF16)
            return 0

        lax.fori_loop(0, HID // 128, step, 0)

    chunks = (pl.ds(0, 1024), pl.ds(1024, 1024))
    top, bot = pl.ds(0, HALF), pl.ds(HALF, HALF)

    def down(i, col):
        return nt_dot(hid[i // 2], wd[col, :])

    phase("up1")
    up(R1, pre)
    phase("d3b")
    g_d.s3((-1, 1))
    phase("d3c")
    g_d.s3((2,))
    g_d.s4((0,))
    phase("conv1")
    conv(R1, pre, ((xat(1), 1), (xat(3), 0)))
    phase("d4a")
    g_d.s4((-1, 1))
    phase("d4b")
    g_d.s4((2,))
    phase("d5")
    g_d.s5()
    phase("down1")
    s_one, s_two, s_three = [], [], []
    for col in chunks:
        a = down(R1, col)
        s1[:, col] = a.astype(BF16)
        s_one.append(push(s1.at[top, col], rl.at[bot, col], right))
        s_one.append(push(s1.at[bot, col], rr.at[top, col], left))

    n_r1.wait_recv()
    put_halo(O0, L1, 0)
    phase("up0a")
    up(O0, pre0, (0,))

    phase("wait_n2")
    f_r.wait_recv()
    f_l.wait_recv()
    nb[A1, 0:HALO, :] = nb[A0, HALF:EXT, :]
    put_halo(A0, R1, 2)
    phase("up2")
    up(A0, pre)
    phase("conv2")
    conv(A0, pre, ((xat(2), 0), (xat(2), 1)))
    phase("down2")
    for col in chunks:
        s2[:, col] = down(A0, col).astype(BF16)
        s_two.append(
            (
                push(s2.at[top, col], tl.at[:, col], right),
                push(s2.at[bot, col], tr.at[:, col], left),
            )
        )

    phase("wait_n1")
    n_l0.wait_recv()
    nb[L1, 0:HALO, :] = nb[L0, HALF:EXT, :]
    put_halo(R0, O1, 3)
    phase("up3")
    up(R0, pre)
    phase("conv3")
    conv(R0, pre, ((xat(1), 0), (xat(3), 1)))
    phase("down3")
    for col in chunks:
        p3[:, col] = down(R0, col)

    def finish(i, col):
        s_two[i][0].wait_recv()
        s3[top, col] = (p3[top, col] + tl[:, col].astype(F32)).astype(BF16)
        s_three.append(push(s3.at[top, col], rl.at[top, col], right))
        s_two[i][1].wait_recv()
        s3[bot, col] = (p3[bot, col] + tr[:, col].astype(F32)).astype(BF16)
        s_three.append(push(s3.at[bot, col], rr.at[bot, col], left))

    phase("wait_t0")
    finish(0, chunks[0])

    phase("up0b")
    up(O0, pre0, (1,))
    phase("conv0")
    conv(O0, pre0, ((x, 0), (x, 1)))
    phase("wait_t1")
    finish(1, chunks[1])
    phase("down0")
    for col in chunks:
        mid[:, col] += down(O0, col)

    phase("wait_s1")
    for cp in s_one:
        cp.wait_recv()
    for i, col in enumerate(chunks):
        phase("wait_s3")
        s_three[2 * i].wait_recv()
        s_three[2 * i + 1].wait_recv()
        phase("final")
        out[:, col] = (mid[:, col] + rl[:, col].astype(F32) + rr[:, col].astype(F32)).astype(BF16)
    phase("wait_sends")
    for cp in copies:
        cp.wait_send()

    @pl.when(x == 3)
    def _():
        for cp in edges:
            cp.wait_send()

    @pl.when(jnp.logical_not(last))
    def _():
        h_kv.wait_send()
        h_drow.wait_send()

    for g in (g_o, g_u, g_d):
        g.gone()
    phase(None)
    assert used["s"] <= N_SEND and used["r"] <= N_RECV, used


def per_device(
    queries,
    keys,
    values,
    doc_ids,
    sinks,
    residual,
    out_weight,
    norm_gain,
    w_gate,
    w_value,
    conv_gate,
    conv_value,
    w_down,
):
    drow = doc_ids.reshape(8, 128)
    wdt = w_down.T
    any_spec = pl.BlockSpec(memory_space=pl.ANY)
    smem = pl.BlockSpec(memory_space=pltpu.SMEM)
    V = pltpu.VMEM
    i32 = jnp.int32
    return pl.pallas_call(
        kernel,
        out_shape=pltpu.VMEM((BLK, D), BF16),
        in_specs=[any_spec] * 4 + [smem] + [any_spec] * 8,
        out_specs=pl.BlockSpec(memory_space=pltpu.VMEM),
        scratch_shapes=[
            V((ROWS, 256), BF16),
            V((128, ROWS + WINDOW), BF16),
            V((ROWS + WINDOW, 2048), BF16),
            V((16, 128), i32),
            V((ROWS + HALO, 128), F32),
            V((ROWS, 128), F32),
            V((ROWS, 128), F32),
            V((ROWS, 256), BF16),
            V((BLK, 1024), BF16),
            V((2, HALF, 256), BF16),
            V((4, 256, D), BF16),
            V((BLK, D), BF16),
            V((BLK, D), F32),
            V((1, D), F32),
            V((8, EXT, D), BF16),
            V((HALO, D), BF16),
            V((D, 2 * HID), BF16),
            V((D, HID), BF16),
            V((PAIR, 2 * HID), F32),
            V((PAIR, 2 * HID), F32),
            V((4, BLK, HID), BF16),
            V((3, HID), F32),
            V((3, HID), F32),
            V((BLK, D), BF16),
            V((BLK, D), BF16),
            V((BLK, D), BF16),
            V((BLK, D), F32),
            V((BLK, D), BF16),
            V((BLK, D), BF16),
            V((128, D), BF16),
            V((128, D), BF16),
            pltpu.SemaphoreType.DMA((N_SEND,)),
            pltpu.SemaphoreType.DMA((N_RECV,)),
            pltpu.SemaphoreType.DMA((16,)),
        ],
        compiler_params=pltpu.CompilerParams(
            collective_id=0,
            has_side_effects=True,
            vmem_limit_bytes=62_000_000,
        ),
        cost_estimate=pl.CostEstimate(
            flops=20_000_000_000, bytes_accessed=10_000_000, transcendentals=4_000_000
        ),
    )(
        queries,
        keys.T,
        values.T,
        drow,
        sinks,
        residual,
        out_weight,
        norm_gain.reshape(1, D),
        w_gate,
        w_value,
        conv_gate,
        conv_value,
        wdt,
    )


def solution(mesh):
    return jax.shard_map(
        per_device,
        mesh=mesh,
        in_specs=(
            P("sp", "tp"),
            P("sp", "tp"),
            P("sp", "tp"),
            P("sp"),
            P("tp"),
            P(("sp", "tp"), None),
            P("tp", None),
            P(),
            P("sp", "tp"),
            P("sp", "tp"),
            P(None, "tp"),
            P(None, "tp"),
            P("tp", "sp"),
        ),
        out_specs=P(("sp", "tp"), None),
        check_vma=False,
    )
```

```python
import functools

import jax
import jax.numpy as jnp
from jax import lax
from jax.experimental import pallas as pl
from jax.experimental.pallas import tpu as pltpu
from jax.sharding import PartitionSpec as P

HEAD_DIM = 64
WINDOW = 128
MESH = pl.DeviceIdType.MESH
F32 = jnp.float32
BF16 = jnp.bfloat16
NT = (((1,), (1,)), ((), ()))

N_SP = 32
ROWS = 1024
BLK = 256
D = 2048
HID = 1408
HALO = 8
HALF = BLK // 2
EXT = HALF + HALO
PAIR = 2 * EXT
N_SEND, N_RECV = 40, 64
R1, L0, R0, L1, O0, O1, A0, A1 = range(8)
POS = {0: 0, 1: 1, 3: 2, 2: 3}
TN = (((0,), (0,)), ((), ()))


def ceil_dot(a, b):
    return jnp.dot(a, b, preferred_element_type=F32)


def nt_dot(a, b):
    return lax.dot_general(a, b, NT, preferred_element_type=F32)


def kernel(
    q_in,
    k_in,
    v_in,
    drow_in,
    sinks,
    res_in,
    ow_in,
    gain_in,
    wg_in,
    wv_in,
    cg_in,
    cv_in,
    wd_in,
    out,
    q,
    kvt,
    kvz,
    drow,
    dcol,
    m1,
    m2,
    att,
    af,
    via,
    ow,
    res,
    mid,
    gain,
    nb,
    edge,
    wu,
    wd,
    pre,
    pre0,
    hid,
    cg,
    cv,
    s1,
    s2,
    s3,
    p3,
    rl,
    rr,
    tl,
    tr,
    send_sem,
    recv_sem,
    loc_sem,
):
    sp = lax.axis_index("sp")
    x = lax.axis_index("tp")
    c = lax.rem(sp, 2)
    k = lax.div(sp, 2)
    y = lax.rem(k, 4)
    z = lax.div(k, 4)

    def sp_of(zz, yy):
        return (lax.rem(zz + 8, 4) * 4 + lax.rem(yy + 8, 4)) * 2 + c

    def xat(j):
        return lax.rem(x + j + 4, 4)

    def dev(s, t):
        return {"sp": s, "tp": t}

    sp_next = lax.rem(sp + 1, N_SP)
    sp_prev = lax.rem(sp + N_SP - 1, N_SP)
    sib = sp + 1 - 2 * c
    right, left = dev(sp, xat(1)), dev(sp, xat(3))

    scopes = []

    def phase(name):
        if scopes:
            scopes.pop().__exit__(None, None, None)
        if name:
            scopes.append(jax.named_scope(name))
            scopes[-1].__enter__()

    phase("local")
    bar = pltpu.get_barrier_semaphore()

    def hello(d):
        pl.semaphore_signal(bar, inc=1, device_id=d, device_id_type=MESH)

    for j in (1, 2, 3):
        hello(dev(sp, xat(j)))
    for dz, dy in ((0, 1), (0, -1), (1, 0), (-1, 0)):
        hello(dev(sp_of(z + dz, y + dy), x))
    hello(dev(sib, x))
    for j in range(4):
        hello(dev(sp_prev, xat(j)))

    loc = []

    def local(src, dst):
        cp = pltpu.make_async_copy(src, dst, loc_sem.at[len(loc)])
        cp.start()
        loc.append(cp)
        return cp

    l_k = local(k_in, kvt.at[pl.ds(0, 64), pl.ds(WINDOW, ROWS)])
    l_v = local(v_in, kvt.at[pl.ds(64, 64), pl.ds(WINDOW, ROWS)])
    l_drow = local(drow_in, drow.at[pl.ds(8, 8)])
    l_ow = local(ow_in, ow.at[0])
    row64 = pl.ds(pl.multiple_of(sp * 64, 64), 64)
    l_wg = local(wg_in, wu.at[row64, pl.ds(0, HID)])
    l_wv = local(wv_in, wu.at[row64, pl.ds(HID, HID)])
    l_q = local(q_in, q)
    l_wd = local(wd_in, wd.at[row64])
    l_res = local(res_in, res)
    l_gain = local(gain_in, gain)
    l_cg = local(cg_in, cg)
    l_cv = local(cv_in, cv)

    phase("barrier")
    pl.semaphore_wait(bar, 12)

    phase("send0")
    copies = []
    used = {"s": 0, "r": 0}

    def new(kind):
        used[kind] += 1
        return (send_sem if kind == "s" else recv_sem).at[used[kind] - 1]

    def push(src, dst, d, ss=None, rs=None):
        cp = pltpu.make_async_remote_copy(
            src_ref=src,
            dst_ref=dst,
            send_sem=new("s") if ss is None else ss,
            recv_sem=new("r") if rs is None else rs,
            device_id=d,
            device_id_type=MESH,
        )
        cp.start()
        if ss is None:
            copies.append(cp)
        return cp

    def wait_all(sem, view):
        pltpu.make_async_copy(view, view, sem).wait()

    l_k.wait()
    l_v.wait()
    l_drow.wait()
    nxt = dev(sp_next, x)
    first = sp == 0
    last = sp == N_SP - 1

    def remote(src, dst, d):
        return pltpu.make_async_remote_copy(
            src_ref=src,
            dst_ref=dst,
            send_sem=new("s"),
            recv_sem=new("r"),
            device_id=d,
            device_id_type=MESH,
        )

    h_kv = remote(kvt.at[:, pl.ds(ROWS, WINDOW)], kvt.at[:, pl.ds(0, WINDOW)], nxt)
    h_drow = remote(drow.at[pl.ds(8, 8)], drow.at[pl.ds(0, 8)], nxt)

    @pl.when(jnp.logical_not(last))
    def _():
        h_kv.start()
        h_drow.start()

    @pl.when(first)
    def _():
        kvt[:, 0:WINDOW] = jnp.zeros((128, WINDOW), BF16)
        drow[0:8, :] = jnp.zeros((8, 128), jnp.int32)

    def wu_view(half, kk, cc, part):
        r = (kk * 2 + cc) * 64
        n = 64 if part is None else 32
        if part == 1:
            r = r + 32
        return wu.at[pl.ds(pl.multiple_of(r, 32), n), pl.ds(half * HID, HID)]

    def wd_view(half, kk, cc, part):
        r = (kk * 2 + cc) * 64 + 32 * half
        n = 32 if part is None else 16
        if part == 1:
            r = r + 16
        return wd.at[pl.ds(pl.multiple_of(r, 16), n)]

    def yz(half, n):
        dy, dz = (n, 0) if half == 0 else (0, n)
        return dev(sp_of(z + dz, y + dy), x)

    class Group:
        def __init__(self, size):
            self.size = size
            self.ss = new("s")
            self.sent = 0
            self.sem = {}
            self.due = {}
            self.held = []

        def go(self, key, ref, units, d, dst=None):
            if key not in self.sem:
                self.sem[key] = new("r")
                self.due[key] = 0
            push(ref, ref if dst is None else dst, d, self.ss, self.sem[key])
            self.due[key] += units
            self.sent += units

        def come(self, key):
            wait_all(self.sem[key], self.size(self.due[key]))

        def share(self, ref, units=2, key="sib"):
            self.go(key, ref, units, dev(sib, x))

        def s5(self):
            self.come("sib")

        def gone(self):
            wait_all(self.ss, self.size(self.sent))

    class Gather(Group):
        def __init__(self, view, size):
            super().__init__(size)
            self.view = view

        def at(self, half, dp, dq, part=None):
            dy, dz = (dp, dq) if half == 0 else (dq, dp)
            kk = lax.rem(z + dz + 8, 4) * 4 + lax.rem(y + dy + 8, 4)
            return self.view(half, kk, c, part)

        def p(self, half, n):
            return yz(half, n)

        def q(self, half, n):
            return yz(1 - half, n)

        def s0p(self):
            for half in (0, 1):
                b = self.at(half, 0, 0)
                self.go("p", b, 2, self.p(half, 1))
                self.go("p", b, 2, self.p(half, -1))

        def s1p(self):
            self.come("p")
            for half in (0, 1):
                self.go("pf", self.at(half, -1, 0, 0), 1, self.p(half, 1))
                self.go("pf", self.at(half, 1, 0, 1), 1, self.p(half, -1))

        def s1q(self, dp, part=None):
            n = 2 if part is None else 1
            for half in (0, 1):
                b = self.at(half, dp, 0, part)
                self.go(("q", dp), b, n, self.q(half, 1))
                self.go(("q", dp), b, n, self.q(half, -1))
                self.held.append((b, n))

        def hand_over(self):
            for b, n in self.held:
                self.share(b, n)
            self.held = []

        def s2(self):
            self.come("pf")
            self.s1q(2)
            if self is not g_u:
                self.hand_over()

        def s3(self, dps):
            for dp in dps:
                self.come(("q", dp))
                for half in (0, 1):
                    lo, hi = self.at(half, dp, -1), self.at(half, dp, 1)
                    if dp in (0, 1):
                        self.go(("f", dp), lo, 2, self.q(half, 1))
                    else:
                        self.go(("f", dp), hi, 2, self.q(half, -1))
                    self.share(lo)
                    self.share(hi)

        def s4(self, dps):
            for dp in dps:
                self.come(("f", dp))
                for half in (0, 1):
                    self.share(self.at(half, dp, 2))

    class GatherOut(Group):
        def at(self, j, par, r, n):
            r = lax.rem(y + z + par, 2) * 128 + r
            cols = pl.ds(pl.multiple_of(c * 1024, 1024), 1024)
            return ow.at[POS[j % 4], pl.ds(pl.multiple_of(r, 32), n), cols]

        def piece(self, j, half):
            return self.at(j, 0, half * 64, 64)

        def over(self, key, j, half, to):
            d = right if to == 1 else left
            self.go(key, self.piece(j, half), 4, d, self.piece(j - to, half))

        def spread(self, j, half, n):
            for i in (0, 1):
                self.go(("y", n), self.at(j, 0, half * 64 + i * 32, 32), 2, yz(half, 1 - 2 * i))
            self.share(self.piece(j, half), 4, ("sib", n == 2))

        def s0(self):
            self.over("x0", 0, 0, 1)
            self.over("x0", 0, 1, -1)
            self.over("x1", 0, 1, 1)
            self.over("x1", 0, 0, -1)

        def s1a(self):
            self.come("x0")
            self.over("xf", 3, 0, 1)
            self.over("xf", 1, 1, -1)
            self.spread(3, 0, 0)
            self.spread(1, 1, 0)

        def s1b(self):
            self.come("x1")
            self.spread(3, 1, 1)
            self.spread(1, 0, 1)

        def s2(self):
            self.come("xf")
            self.spread(2, 0, 2)
            self.spread(2, 1, 2)

        def s4(self, n):
            self.come(("y", n))
            for j, half in (((3, 0), (1, 1)), ((3, 1), (1, 0)), ((2, 0), (2, 1)))[n]:
                self.share(self.at(j, 1, half * 64, 64), 4, ("sib", n == 2))

    def ow_size(n):
        for quarters in (1, 2, 3, 4):
            if n * 8 % quarters == 0 and n * 8 // quarters <= 256:
                return ow.at[pl.ds(0, quarters), pl.ds(0, n * 8 // quarters)]

    g_o = GatherOut(ow_size)
    g_u = Gather(wu_view, lambda n: wu.at[pl.ds(0, 16 * n)])
    g_d = Gather(wd_view, lambda n: wd.at[pl.ds(0, 16 * n)])

    l_ow.wait()
    g_o.s0()
    l_wg.wait()
    l_wv.wait()
    g_u.s0p()
    l_wd.wait()
    g_d.s0p()

    phase("column")
    er = lax.broadcasted_iota(jnp.int32, (128, 2048), 0)
    ec = lax.broadcasted_iota(jnp.int32, (128, 2048), 1)
    sel = (
        ((er >> 6) == (ec >> 10))
        & ((er & 63) == (ec & 63))
        & (((ec >> 8) & 3) == ((ec >> 6) & 3))
    )
    place = jnp.where(sel, 1.0, 0.0).astype(BF16)

    def column(i, _):
        r = pl.ds(pl.multiple_of(HALO + i * 128, 8), 128)
        dcol[r, :] = jnp.broadcast_to(drow[pl.ds(8 + i, 1), :].astype(F32), (128, 128)).T
        return 0

    lax.fori_loop(0, 8, column, 0)

    phase("expand")

    def expand(i, _):
        r = pl.ds(pl.multiple_of(i * 128, 128), 128)
        kvz[r, :] = lax.dot_general(kvt[:, r], place, TN, preferred_element_type=F32).astype(BF16)
        return 0

    lax.fori_loop(1, 9, expand, 0)
    phase("wait_halo")

    @pl.when(jnp.logical_not(first))
    def _():
        h_kv.wait_recv()
        h_drow.wait_recv()

    phase("masks")
    expand(0, 0)
    ahead = jnp.broadcast_to(drow[7:8, :].astype(F32), (128, 128)).T
    dcol[0:HALO, :] = ahead[128 - HALO :, :]

    t_ids = lax.broadcasted_iota(jnp.int32, (ROWS, 128), 0)
    center = dcol[HALO : HALO + ROWS, :]
    ok1 = (dcol[HALO - 1 : HALO - 1 + ROWS, :] == center) & ((t_ids >= 1) | jnp.logical_not(first))
    ok2 = (dcol[HALO - 2 : HALO - 2 + ROWS, :] == center) & ((t_ids >= 2) | jnp.logical_not(first))
    m1[...] = jnp.where(ok1, 1.0, 0.0)
    m2[...] = jnp.where(ok2, 1.0, 0.0)

    l_q.wait()

    ri = lax.broadcasted_iota(jnp.int32, (128, 128), 0)
    ci = lax.broadcasted_iota(jnp.int32, (128, 128), 1)

    def attend(b):
        r0 = pl.multiple_of(b * 128, 128)
        qb = q[pl.ds(r0, 128), :]
        keys = pl.ds(r0, 256)
        dq = dcol[pl.ds(pl.multiple_of(HALO + b * 128, 8), 128), :]
        k0 = drow[pl.ds(7 + b, 1), :].astype(F32)
        k1 = drow[pl.ds(8 + b, 1), :].astype(F32)
        there = jnp.logical_not(first & (b == 0))
        lower = (dq == k0) & (ci > ri) & there
        upper = (dq == k1) & (ci <= ri)
        keep = jnp.concatenate([lower, upper], axis=1)
        o = jnp.zeros((128, 256), F32)
        for h in range(4):
            s = nt_dot(qb, kvz[keys, h * 256 : (h + 1) * 256]) * (HEAD_DIM**-0.5)
            s = jnp.where(keep, s, -jnp.inf)
            sink = sinks[h]
            peak = jnp.maximum(jnp.max(s, axis=-1, keepdims=True), sink)
            e = jnp.exp(s - peak)
            total = jnp.sum(e, axis=-1, keepdims=True) + jnp.exp(sink - peak)
            p = (e / total).astype(BF16)
            o = o + ceil_dot(p, kvz[keys, 1024 + h * 256 : 1024 + (h + 1) * 256])
        att[pl.ds(r0, 128), :] = o.astype(BF16)

    a2a, over, across = {}, [], []

    def af_col(j):
        return af.at[:, pl.ds(POS[(-j) % 4] * 256, 256)]

    for j in (2, 1, 3, 0):
        t = xat(j)

        def two(i, _, t=t):
            attend(t * 2 + i)
            return 0

        if j == 0:
            phase("o2")
            g_o.s2()
        phase(f"attend{j}")
        lax.fori_loop(0, 2, two, 0)
        rows = att.at[pl.ds(pl.multiple_of(t * 256, 256), 256)]
        if j == 2:
            for h, d in ((0, right), (1, left)):
                half = att.at[pl.ds(pl.multiple_of(t * 256 + h * 128, 128), 128)]
                over.append(push(half, via.at[h], d))
        elif j:
            a2a[j] = push(rows, af_col(j), dev(sp, t))
        else:
            l_af = local(rows, af_col(0))
        if j == 2:
            phase("o1a")
            g_o.s1a()
            phase("d0p")
            g_u.s1q(0, 0)
        if j == 1:
            phase("o1b")
            g_o.s1b()
            phase("u1p")
            g_u.s1p()
        if j == 3:
            phase("a2f")
            for h, d in ((0, right), (1, left)):
                over[h].wait_recv()
                across.append(push(via.at[h], af_col(2).at[pl.ds(h * 128, 128)], d))
    phase("u1")
    g_u.s1q(0, 1)
    g_u.s1q(-1)
    g_u.s1q(1)
    g_o.s4(0)
    phase("o4a")
    g_o.s4(1)
    g_d.s1p()
    phase("a2a")
    l_af.wait()
    for cp in (a2a[1], a2a[3], *across):
        cp.wait_recv()
    l_res.wait()
    l_gain.wait()
    l_cg.wait()
    l_cv.wait()
    phase("o5a")
    g_o.come(("sib", False))

    phase("project1")

    def project1(j, _):
        col = pl.ds(pl.multiple_of(j * 512, 512), 512)
        w = ow[0:3, :, col].reshape(768, 512)
        mid[:, col] = res[:, col].astype(F32) + ceil_dot(af[:, 0:768], w)
        return 0

    lax.fori_loop(0, D // 512, project1, 0)
    phase("o4b")
    g_o.s4(2)
    phase("u2")
    g_u.s2()
    phase("o5b")
    g_o.come(("sib", True))
    phase("project2")

    def project2(j, sq):
        col = pl.ds(pl.multiple_of(j * 512, 512), 512)
        m = mid[:, col] + ceil_dot(af[:, 768:1024], ow[3, :, col])
        m = m.astype(BF16).astype(F32)
        mid[:, col] = m
        return sq + jnp.sum(m * m, axis=-1, keepdims=True)

    sq = lax.fori_loop(0, D // 512, project2, jnp.zeros((BLK, 1), F32))
    inv = lax.rsqrt(sq * (1.0 / D) + 1e-06)
    for h in (0, 1):
        r = slice(h * HALF, (h + 1) * HALF)
        for j in range(D // 512):
            col = slice(j * 512, (j + 1) * 512)
            n = (mid[r, col] * inv[r] * gain[:, col]).astype(BF16)
            nb[O0 + h, HALO:EXT, col] = n
            if h == 0:
                nb[O1, 0:HALO, col] = n[HALF - HALO :]

    phase("send_n")

    def rows_of(i):
        return nb.at[i, pl.ds(HALO, HALF)]

    def halo_of(i):
        return nb.at[i, pl.ds(0, HALO)]

    tail = nb.at[O1, pl.ds(HALF, HALO)]
    n_mid = push(halo_of(O1), halo_of(R1), left)
    n_r0 = push(rows_of(O0), rows_of(L0), right)
    n_l1 = push(rows_of(O1), rows_of(R1), left)
    tails = [push(tail, halo_of(L0), dev(jnp.where(x == 3, sp_next, sp), xat(2)))]
    edges = [remote(tail, edge, dev(sp_next, xat(j))) for j in (0, 1, 3)]
    edge_from = {0: 3, 1: 0, 3: 2}

    @pl.when(x == 3)
    def _():
        for cp in edges:
            cp.start()

    n_r1 = push(rows_of(O1), rows_of(L1), right)
    n_l0 = push(rows_of(O0), rows_of(R0), left)

    g_u.hand_over()
    phase("u3a")
    g_u.s3((0,))
    phase("u3b")
    g_u.s3((-1,))
    phase("u3c")
    g_u.s3((1,))
    g_d.s1q(0)
    phase("u3d")
    g_u.s3((2,))
    g_d.s1q(-1)
    g_d.s1q(1)
    phase("d2")
    g_d.s2()
    phase("u4a")
    g_u.s4((0, -1))
    phase("n_half")
    n_r0.wait_recv()
    f_r = push(rows_of(L0), rows_of(A0), right)
    n_l1.wait_recv()
    f_l = push(rows_of(R1), rows_of(A1), left)
    phase("u4c")
    g_u.s4((1, 2))
    phase("d3a")
    g_d.s3((0,))
    phase("u5")
    g_u.s5()
    phase("tails")
    n_mid.wait_recv()
    for cp in tails:
        cp.wait_recv()
    for j, cp in zip((0, 1, 3), edges):

        @pl.when(x == edge_from[j])
        def _(cp=cp):
            cp.wait_recv()

    def put_halo(slot, before, edge_x):
        near = nb[before, HALF:EXT, :]
        nb[slot, 0:HALO, :] = jnp.where(x == edge_x, edge[...], near)

    def up(i, to, parts=(0, 1)):
        rows = nb[i : i + 2].reshape(PAIR, D)
        for h in parts:
            col = pl.ds(h * HID, HID)
            to[:, col] = ceil_dot(rows, wu[:, col]).astype(BF16).astype(F32)

    def conv(i, pre, blocks):
        def step(j, _):
            gc = pl.ds(pl.multiple_of(j * 128, 128), 128)
            vc = pl.ds(pl.multiple_of(HID + j * 128, 128), 128)
            tg = cg[:, gc]
            tv = cv[:, gc]
            for n, (d, h) in enumerate(blocks):
                for r in range(0, HALF, 64):
                    mr = pl.ds(pl.multiple_of(d * BLK + h * HALF + r, 64), 64)
                    k1 = m1[mr, :] > 0.5
                    k2 = m2[mr, :] > 0.5
                    r0 = n * EXT + HALO + r

                    def taps(t, cc):
                        a = t[2:3] * pre[r0 : r0 + 64, cc]
                        a = a + jnp.where(k1, t[1:2] * pre[r0 - 1 : r0 + 63, cc], 0.0)
                        return a + jnp.where(k2, t[0:1] * pre[r0 - 2 : r0 + 62, cc], 0.0)

                    g = taps(tg, gc)
                    v = taps(tv, vc)
                    o = n * HALF + r
                    hid[i // 2, o : o + 64, gc] = (g / (1.0 + jnp.exp(-g)) * v).astype(BF16)
            return 0

        lax.fori_loop(0, HID // 128, step, 0)

    chunks = (pl.ds(0, 1024), pl.ds(1024, 1024))
    top, bot = pl.ds(0, HALF), pl.ds(HALF, HALF)

    def down(i, col):
        return nt_dot(hid[i // 2], wd[col, :])

    phase("up1")
    up(R1, pre, (0,))
    phase("d3b")
    g_d.s3((-1,))
    phase("up1b")
    up(R1, pre, (1,))
    phase("d3b2")
    g_d.s3((1,))
    phase("d3c")
    g_d.s3((2,))
    g_d.s4((0,))
    phase("conv1")
    conv(R1, pre, ((xat(1), 1), (xat(3), 0)))
    phase("d4a")
    g_d.s4((-1, 1))
    phase("d4b")
    g_d.s4((2,))
    phase("d5")
    g_d.s5()
    phase("down1")
    s_one, s_two, s_three = [], [], []
    for col in chunks:
        a = down(R1, col)
        s1[:, col] = a.astype(BF16)
        s_one.append(push(s1.at[top, col], rl.at[bot, col], right))
        s_one.append(push(s1.at[bot, col], rr.at[top, col], left))

    n_r1.wait_recv()
    put_halo(O0, L1, 0)
    phase("up0a")
    up(O0, pre0, (0,))

    phase("wait_n2")
    f_r.wait_recv()
    f_l.wait_recv()
    nb[A1, 0:HALO, :] = nb[A0, HALF:EXT, :]
    put_halo(A0, R1, 2)
    phase("up2")
    up(A0, pre)
    phase("conv2")
    conv(A0, pre, ((xat(2), 0), (xat(2), 1)))
    phase("down2")
    for col in chunks:
        s2[:, col] = down(A0, col).astype(BF16)
        s_two.append(
            (
                push(s2.at[top, col], tl.at[:, col], right),
                push(s2.at[bot, col], tr.at[:, col], left),
            )
        )

    phase("wait_n1")
    n_l0.wait_recv()
    nb[L1, 0:HALO, :] = nb[L0, HALF:EXT, :]
    put_halo(R0, O1, 3)
    phase("up3")
    up(R0, pre)
    phase("conv3")
    conv(R0, pre, ((xat(1), 0), (xat(3), 1)))
    phase("down3")
    for col in chunks:
        p3[:, col] = down(R0, col)

    def finish(i, col):
        s_two[i][0].wait_recv()
        s3[top, col] = (p3[top, col] + tl[:, col].astype(F32)).astype(BF16)
        s_three.append(push(s3.at[top, col], rl.at[top, col], right))
        s_two[i][1].wait_recv()
        s3[bot, col] = (p3[bot, col] + tr[:, col].astype(F32)).astype(BF16)
        s_three.append(push(s3.at[bot, col], rr.at[bot, col], left))

    phase("wait_t0")
    finish(0, chunks[0])

    phase("up0b")
    up(O0, pre0, (1,))
    phase("conv0")
    conv(O0, pre0, ((x, 0), (x, 1)))
    phase("wait_t1")
    finish(1, chunks[1])
    phase("down0")
    for col in chunks:
        mid[:, col] += down(O0, col)

    phase("wait_s1")
    for cp in s_one:
        cp.wait_recv()
    for i, col in enumerate(chunks):
        phase("wait_s3")
        s_three[2 * i].wait_recv()
        s_three[2 * i + 1].wait_recv()
        phase("final")
        out[:, col] = (mid[:, col] + rl[:, col].astype(F32) + rr[:, col].astype(F32)).astype(BF16)
    phase("wait_sends")
    for cp in copies:
        cp.wait_send()

    @pl.when(x == 3)
    def _():
        for cp in edges:
            cp.wait_send()

    @pl.when(jnp.logical_not(last))
    def _():
        h_kv.wait_send()
        h_drow.wait_send()

    for g in (g_o, g_u, g_d):
        g.gone()
    phase(None)
    assert used["s"] <= N_SEND and used["r"] <= N_RECV, used


def per_device(
    queries,
    keys,
    values,
    doc_ids,
    sinks,
    residual,
    out_weight,
    norm_gain,
    w_gate,
    w_value,
    conv_gate,
    conv_value,
    w_down,
):
    drow = doc_ids.reshape(8, 128)
    wdt = w_down.T
    any_spec = pl.BlockSpec(memory_space=pl.ANY)
    smem = pl.BlockSpec(memory_space=pltpu.SMEM)
    V = pltpu.VMEM
    i32 = jnp.int32
    return pl.pallas_call(
        kernel,
        out_shape=pltpu.VMEM((BLK, D), BF16),
        in_specs=[any_spec] * 4 + [smem] + [any_spec] * 8,
        out_specs=pl.BlockSpec(memory_space=pltpu.VMEM),
        scratch_shapes=[
            V((ROWS, 256), BF16),
            V((128, ROWS + WINDOW), BF16),
            V((ROWS + WINDOW, 2048), BF16),
            V((16, 128), i32),
            V((ROWS + HALO, 128), F32),
            V((ROWS, 128), F32),
            V((ROWS, 128), F32),
            V((ROWS, 256), BF16),
            V((BLK, 1024), BF16),
            V((2, HALF, 256), BF16),
            V((4, 256, D), BF16),
            V((BLK, D), BF16),
            V((BLK, D), F32),
            V((1, D), F32),
            V((8, EXT, D), BF16),
            V((HALO, D), BF16),
            V((D, 2 * HID), BF16),
            V((D, HID), BF16),
            V((PAIR, 2 * HID), F32),
            V((PAIR, 2 * HID), F32),
            V((4, BLK, HID), BF16),
            V((3, HID), F32),
            V((3, HID), F32),
            V((BLK, D), BF16),
            V((BLK, D), BF16),
            V((BLK, D), BF16),
            V((BLK, D), F32),
            V((BLK, D), BF16),
            V((BLK, D), BF16),
            V((128, D), BF16),
            V((128, D), BF16),
            pltpu.SemaphoreType.DMA((N_SEND,)),
            pltpu.SemaphoreType.DMA((N_RECV,)),
            pltpu.SemaphoreType.DMA((16,)),
        ],
        compiler_params=pltpu.CompilerParams(
            collective_id=0,
            has_side_effects=True,
            vmem_limit_bytes=62_000_000,
        ),
        cost_estimate=pl.CostEstimate(
            flops=20_000_000_000, bytes_accessed=10_000_000, transcendentals=4_000_000
        ),
    )(
        queries,
        keys.T,
        values.T,
        drow,
        sinks,
        residual,
        out_weight,
        norm_gain.reshape(1, D),
        w_gate,
        w_value,
        conv_gate,
        conv_value,
        wdt,
    )


def solution(mesh):
    return jax.shard_map(
        per_device,
        mesh=mesh,
        in_specs=(
            P("sp", "tp"),
            P("sp", "tp"),
            P("sp", "tp"),
            P("sp"),
            P("tp"),
            P(("sp", "tp"), None),
            P("tp", None),
            P(),
            P("sp", "tp"),
            P("sp", "tp"),
            P(None, "tp"),
            P(None, "tp"),
            P("tp", "sp"),
        ),
        out_specs=P(("sp", "tp"), None),
        check_vma=False,
    )
```

```python
import functools

import jax
import jax.numpy as jnp
from jax import lax
from jax.experimental import pallas as pl
from jax.experimental.pallas import tpu as pltpu
from jax.sharding import PartitionSpec as P

HEAD_DIM = 64
WINDOW = 128
MESH = pl.DeviceIdType.MESH
F32 = jnp.float32
BF16 = jnp.bfloat16
NT = (((1,), (1,)), ((), ()))

N_SP = 32
ROWS = 1024
BLK = 256
D = 2048
HID = 1408
HALO = 8
HALF = BLK // 2
EXT = HALF + HALO
PAIR = 2 * EXT
N_SEND, N_RECV = 40, 64
R1, L0, R0, L1, O0, O1, A0, A1 = range(8)
POS = {0: 0, 1: 1, 3: 2, 2: 3}
TN = (((0,), (0,)), ((), ()))


def ceil_dot(a, b):
    return jnp.dot(a, b, preferred_element_type=F32)


def nt_dot(a, b):
    return lax.dot_general(a, b, NT, preferred_element_type=F32)


def kernel(
    q_in,
    k_in,
    v_in,
    drow_in,
    sinks,
    res_in,
    ow_in,
    gain_in,
    wg_in,
    wv_in,
    cg_in,
    cv_in,
    wd_in,
    out,
    q,
    kvt,
    kvz,
    drow,
    dcol,
    m1,
    m2,
    att,
    af,
    via,
    ow,
    res,
    mid,
    gain,
    nb,
    edge,
    wu,
    wd,
    pre,
    pre0,
    hid,
    cg,
    cv,
    s1,
    s2,
    s3,
    p3,
    rl,
    rr,
    tl,
    tr,
    send_sem,
    recv_sem,
    loc_sem,
):
    sp = lax.axis_index("sp")
    x = lax.axis_index("tp")
    c = lax.rem(sp, 2)
    k = lax.div(sp, 2)
    y = lax.rem(k, 4)
    z = lax.div(k, 4)

    def sp_of(zz, yy):
        return (lax.rem(zz + 8, 4) * 4 + lax.rem(yy + 8, 4)) * 2 + c

    def xat(j):
        return lax.rem(x + j + 4, 4)

    def dev(s, t):
        return {"sp": s, "tp": t}

    sp_next = lax.rem(sp + 1, N_SP)
    sp_prev = lax.rem(sp + N_SP - 1, N_SP)
    sib = sp + 1 - 2 * c
    right, left = dev(sp, xat(1)), dev(sp, xat(3))

    scopes = []

    def phase(name):
        if scopes:
            scopes.pop().__exit__(None, None, None)
        if name:
            scopes.append(jax.named_scope(name))
            scopes[-1].__enter__()

    phase("local")
    bar = pltpu.get_barrier_semaphore()

    def hello(d):
        pl.semaphore_signal(bar, inc=1, device_id=d, device_id_type=MESH)

    for j in (1, 2, 3):
        hello(dev(sp, xat(j)))
    for dz, dy in ((0, 1), (0, -1), (1, 0), (-1, 0)):
        hello(dev(sp_of(z + dz, y + dy), x))
    hello(dev(sib, x))
    for j in range(4):
        hello(dev(sp_prev, xat(j)))

    loc = []

    def local(src, dst):
        cp = pltpu.make_async_copy(src, dst, loc_sem.at[len(loc)])
        cp.start()
        loc.append(cp)
        return cp

    l_k = local(k_in, kvt.at[pl.ds(0, 64), pl.ds(WINDOW, ROWS)])
    l_v = local(v_in, kvt.at[pl.ds(64, 64), pl.ds(WINDOW, ROWS)])
    l_drow = local(drow_in, drow.at[pl.ds(8, 8)])
    l_ow = local(ow_in, ow.at[0])
    row64 = pl.ds(pl.multiple_of(sp * 64, 64), 64)
    l_wg = local(wg_in, wu.at[row64, pl.ds(0, HID)])
    l_wv = local(wv_in, wu.at[row64, pl.ds(HID, HID)])
    l_q = local(q_in, q)
    l_wd = local(wd_in, wd.at[row64])
    l_res = local(res_in, res)
    l_gain = local(gain_in, gain)
    l_cg = local(cg_in, cg)
    l_cv = local(cv_in, cv)

    phase("barrier")
    pl.semaphore_wait(bar, 12)

    phase("send0")
    copies = []
    used = {"s": 0, "r": 0}

    def new(kind):
        used[kind] += 1
        return (send_sem if kind == "s" else recv_sem).at[used[kind] - 1]

    def push(src, dst, d, ss=None, rs=None):
        cp = pltpu.make_async_remote_copy(
            src_ref=src,
            dst_ref=dst,
            send_sem=new("s") if ss is None else ss,
            recv_sem=new("r") if rs is None else rs,
            device_id=d,
            device_id_type=MESH,
        )
        cp.start()
        if ss is None:
            copies.append(cp)
        return cp

    def wait_all(sem, view):
        pltpu.make_async_copy(view, view, sem).wait()

    l_k.wait()
    l_v.wait()
    l_drow.wait()
    nxt = dev(sp_next, x)
    first = sp == 0
    last = sp == N_SP - 1

    def remote(src, dst, d):
        return pltpu.make_async_remote_copy(
            src_ref=src,
            dst_ref=dst,
            send_sem=new("s"),
            recv_sem=new("r"),
            device_id=d,
            device_id_type=MESH,
        )

    h_kv = remote(kvt.at[:, pl.ds(ROWS, WINDOW)], kvt.at[:, pl.ds(0, WINDOW)], nxt)
    h_drow = remote(drow.at[pl.ds(8, 8)], drow.at[pl.ds(0, 8)], nxt)

    @pl.when(jnp.logical_not(last))
    def _():
        h_kv.start()
        h_drow.start()

    @pl.when(first)
    def _():
        kvt[:, 0:WINDOW] = jnp.zeros((128, WINDOW), BF16)
        drow[0:8, :] = jnp.zeros((8, 128), jnp.int32)

    def wu_view(half, kk, cc, part):
        r = (kk * 2 + cc) * 64
        n = 64 if part is None else 32
        if part == 1:
            r = r + 32
        return wu.at[pl.ds(pl.multiple_of(r, 32), n), pl.ds(half * HID, HID)]

    def wd_view(half, kk, cc, part):
        r = (kk * 2 + cc) * 64 + 32 * half
        n = 32 if part is None else 16
        if part == 1:
            r = r + 16
        return wd.at[pl.ds(pl.multiple_of(r, 16), n)]

    def yz(half, n):
        dy, dz = (n, 0) if half == 0 else (0, n)
        return dev(sp_of(z + dz, y + dy), x)

    class Group:
        def __init__(self, size):
            self.size = size
            self.ss = new("s")
            self.sent = 0
            self.sem = {}
            self.due = {}

        def go(self, key, ref, units, d, dst=None):
            if key not in self.sem:
                self.sem[key] = new("r")
                self.due[key] = 0
            push(ref, ref if dst is None else dst, d, self.ss, self.sem[key])
            self.due[key] += units
            self.sent += units

        def come(self, key):
            wait_all(self.sem[key], self.size(self.due[key]))

        def share(self, ref, units=2, key="sib"):
            self.go(key, ref, units, dev(sib, x))

        def s5(self):
            self.come("sib")

        def gone(self):
            wait_all(self.ss, self.size(self.sent))

    class Gather(Group):
        def __init__(self, view, size):
            super().__init__(size)
            self.view = view

        def at(self, half, dp, dq, part=None):
            dy, dz = (dp, dq) if half == 0 else (dq, dp)
            kk = lax.rem(z + dz + 8, 4) * 4 + lax.rem(y + dy + 8, 4)
            return self.view(half, kk, c, part)

        def p(self, half, n):
            return yz(half, n)

        def q(self, half, n):
            return yz(1 - half, n)

        def s0p(self):
            for half in (0, 1):
                b = self.at(half, 0, 0)
                self.go("p", b, 2, self.p(half, 1))
                self.go("p", b, 2, self.p(half, -1))

        def s1p(self):
            self.come("p")
            for half in (0, 1):
                self.go("pf", self.at(half, -1, 0, 0), 1, self.p(half, 1))
                self.go("pf", self.at(half, 1, 0, 1), 1, self.p(half, -1))

        def s1q(self, dp, part=None):
            n = 2 if part is None else 1
            for half in (0, 1):
                b = self.at(half, dp, 0, part)
                self.go(("q", dp), b, n, self.q(half, 1))
                self.go(("q", dp), b, n, self.q(half, -1))
                self.share(b, n)

        def s2(self):
            self.come("pf")
            self.s1q(2)

        def s3(self, dps):
            for dp in dps:
                self.come(("q", dp))
                for half in (0, 1):
                    lo, hi = self.at(half, dp, -1), self.at(half, dp, 1)
                    if dp in (0, 1):
                        self.go(("f", dp), lo, 2, self.q(half, 1))
                    else:
                        self.go(("f", dp), hi, 2, self.q(half, -1))
                    self.share(lo)
                    self.share(hi)

        def s4(self, dps):
            for dp in dps:
                self.come(("f", dp))
                for half in (0, 1):
                    self.share(self.at(half, dp, 2))

    class GatherOut(Group):
        def at(self, j, par, r, n):
            r = lax.rem(y + z + par, 2) * 128 + r
            cols = pl.ds(pl.multiple_of(c * 1024, 1024), 1024)
            return ow.at[POS[j % 4], pl.ds(pl.multiple_of(r, 32), n), cols]

        def piece(self, j, half):
            return self.at(j, 0, half * 64, 64)

        def over(self, key, j, half, to):
            d = right if to == 1 else left
            self.go(key, self.piece(j, half), 4, d, self.piece(j - to, half))

        def spread(self, j, half, n):
            for i in (0, 1):
                self.go(("y", n), self.at(j, 0, half * 64 + i * 32, 32), 2, yz(half, 1 - 2 * i))
            self.share(self.piece(j, half), 4, ("sib", n == 2))

        def s0(self):
            self.over("x0", 0, 0, 1)
            self.over("x0", 0, 1, -1)
            self.over("x1", 0, 1, 1)
            self.over("x1", 0, 0, -1)

        def s1a(self):
            self.come("x0")
            self.over("xf", 3, 0, 1)
            self.over("xf", 1, 1, -1)
            self.spread(3, 0, 0)
            self.spread(1, 1, 0)

        def s1b(self):
            self.come("x1")
            self.spread(3, 1, 1)
            self.spread(1, 0, 1)

        def s2(self):
            self.come("xf")
            self.spread(2, 0, 2)
            self.spread(2, 1, 2)

        def s4(self, n):
            self.come(("y", n))
            for j, half in (((3, 0), (1, 1)), ((3, 1), (1, 0)), ((2, 0), (2, 1)))[n]:
                self.share(self.at(j, 1, half * 64, 64), 4, ("sib", n == 2))

    def ow_size(n):
        for quarters in (1, 2, 3, 4):
            if n * 8 % quarters == 0 and n * 8 // quarters <= 256:
                return ow.at[pl.ds(0, quarters), pl.ds(0, n * 8 // quarters)]

    g_o = GatherOut(ow_size)
    g_u = Gather(wu_view, lambda n: wu.at[pl.ds(0, 16 * n)])
    g_d = Gather(wd_view, lambda n: wd.at[pl.ds(0, 16 * n)])

    l_ow.wait()
    g_o.s0()
    l_wg.wait()
    l_wv.wait()
    g_u.s0p()

    phase("column")
    er = lax.broadcasted_iota(jnp.int32, (128, 2048), 0)
    ec = lax.broadcasted_iota(jnp.int32, (128, 2048), 1)
    sel = (
        ((er >> 6) == (ec >> 10))
        & ((er & 63) == (ec & 63))
        & (((ec >> 8) & 3) == ((ec >> 6) & 3))
    )
    place = jnp.where(sel, 1.0, 0.0).astype(BF16)

    def column(i, _):
        r = pl.ds(pl.multiple_of(HALO + i * 128, 8), 128)
        dcol[r, :] = jnp.broadcast_to(drow[pl.ds(8 + i, 1), :].astype(F32), (128, 128)).T
        return 0

    lax.fori_loop(0, 8, column, 0)

    phase("expand")

    def expand(i, _):
        r = pl.ds(pl.multiple_of(i * 128, 128), 128)
        kvz[r, :] = lax.dot_general(kvt[:, r], place, TN, preferred_element_type=F32).astype(BF16)
        return 0

    lax.fori_loop(1, 9, expand, 0)
    phase("wait_halo")

    @pl.when(jnp.logical_not(first))
    def _():
        h_kv.wait_recv()
        h_drow.wait_recv()

    phase("masks")
    expand(0, 0)
    ahead = jnp.broadcast_to(drow[7:8, :].astype(F32), (128, 128)).T
    dcol[0:HALO, :] = ahead[128 - HALO :, :]

    t_ids = lax.broadcasted_iota(jnp.int32, (ROWS, 128), 0)
    center = dcol[HALO : HALO + ROWS, :]
    ok1 = (dcol[HALO - 1 : HALO - 1 + ROWS, :] == center) & ((t_ids >= 1) | jnp.logical_not(first))
    ok2 = (dcol[HALO - 2 : HALO - 2 + ROWS, :] == center) & ((t_ids >= 2) | jnp.logical_not(first))
    m1[...] = jnp.where(ok1, 1.0, 0.0)
    m2[...] = jnp.where(ok2, 1.0, 0.0)

    l_q.wait()

    ri = lax.broadcasted_iota(jnp.int32, (128, 128), 0)
    ci = lax.broadcasted_iota(jnp.int32, (128, 128), 1)

    def attend(b):
        r0 = pl.multiple_of(b * 128, 128)
        qb = q[pl.ds(r0, 128), :]
        keys = pl.ds(r0, 256)
        dq = dcol[pl.ds(pl.multiple_of(HALO + b * 128, 8), 128), :]
        k0 = drow[pl.ds(7 + b, 1), :].astype(F32)
        k1 = drow[pl.ds(8 + b, 1), :].astype(F32)
        there = jnp.logical_not(first & (b == 0))
        lower = (dq == k0) & (ci > ri) & there
        upper = (dq == k1) & (ci <= ri)
        keep = jnp.concatenate([lower, upper], axis=1)
        o = jnp.zeros((128, 256), F32)
        for h in range(4):
            s = nt_dot(qb, kvz[keys, h * 256 : (h + 1) * 256]) * (HEAD_DIM**-0.5)
            s = jnp.where(keep, s, -jnp.inf)
            sink = sinks[h]
            peak = jnp.maximum(jnp.max(s, axis=-1, keepdims=True), sink)
            e = jnp.exp(s - peak)
            total = jnp.sum(e, axis=-1, keepdims=True) + jnp.exp(sink - peak)
            p = (e / total).astype(BF16)
            o = o + ceil_dot(p, kvz[keys, 1024 + h * 256 : 1024 + (h + 1) * 256])
        att[pl.ds(r0, 128), :] = o.astype(BF16)

    a2a, over, across = {}, [], []

    def af_col(j):
        return af.at[:, pl.ds(POS[(-j) % 4] * 256, 256)]

    for j in (2, 1, 3, 0):
        t = xat(j)

        def two(i, _, t=t):
            attend(t * 2 + i)
            return 0

        phase(f"attend{j}")
        lax.fori_loop(0, 2, two, 0)
        rows = att.at[pl.ds(pl.multiple_of(t * 256, 256), 256)]
        if j == 2:
            for h, d in ((0, right), (1, left)):
                half = att.at[pl.ds(pl.multiple_of(t * 256 + h * 128, 128), 128)]
                over.append(push(half, via.at[h], d))
        elif j:
            a2a[j] = push(rows, af_col(j), dev(sp, t))
        else:
            l_af = local(rows, af_col(0))
        if j == 2:
            phase("o1a")
            g_o.s1a()
            phase("d0p")
            l_wd.wait()
            g_d.s0p()
        if j == 1:
            phase("o1b")
            g_o.s1b()
        if j == 3:
            phase("a2f")
            for h, d in ((0, right), (1, left)):
                over[h].wait_recv()
                across.append(push(via.at[h], af_col(2).at[pl.ds(h * 128, 128)], d))
            phase("u1p")
            g_u.s1p()
    phase("o2")
    g_o.s2()
    phase("u1")
    g_u.s1q(0)
    g_u.s1q(-1)
    g_u.s1q(1)
    g_o.s4(0)
    phase("o4a")
    g_o.s4(1)
    g_d.s1p()
    phase("a2a")
    l_af.wait()
    for cp in (a2a[1], a2a[3], *across):
        cp.wait_recv()
    l_res.wait()
    l_gain.wait()
    l_cg.wait()
    l_cv.wait()
    phase("o5a")
    g_o.come(("sib", False))

    phase("project1")

    def project1(j, _):
        col = pl.ds(pl.multiple_of(j * 512, 512), 512)
        w = ow[0:3, :, col].reshape(768, 512)
        mid[:, col] = res[:, col].astype(F32) + ceil_dot(af[:, 0:768], w)
        return 0

    lax.fori_loop(0, D // 512, project1, 0)
    phase("o4b")
    g_o.s4(2)
    phase("u2")
    g_u.s2()
    phase("o5b")
    g_o.come(("sib", True))
    phase("project2")

    def project2(j, sq):
        col = pl.ds(pl.multiple_of(j * 512, 512), 512)
        m = mid[:, col] + ceil_dot(af[:, 768:1024], ow[3, :, col])
        m = m.astype(BF16).astype(F32)
        mid[:, col] = m
        return sq + jnp.sum(m * m, axis=-1, keepdims=True)

    sq = lax.fori_loop(0, D // 512, project2, jnp.zeros((BLK, 1), F32))
    inv = lax.rsqrt(sq * (1.0 / D) + 1e-06)
    def rows_of(i):
        return nb.at[i, pl.ds(HALO, HALF)]

    def halo_of(i):
        return nb.at[i, pl.ds(0, HALO)]

    for h in (0, 1):
        r = slice(h * HALF, (h + 1) * HALF)
        for j in range(D // 512):
            col = slice(j * 512, (j + 1) * 512)
            n = (mid[r, col] * inv[r] * gain[:, col]).astype(BF16)
            nb[O0 + h, HALO:EXT, col] = n
            if h == 0:
                nb[O1, 0:HALO, col] = n[HALF - HALO :]
        if h == 0:
            n_r0 = push(rows_of(O0), rows_of(L0), right)

    phase("send_n")

    tail = nb.at[O1, pl.ds(HALF, HALO)]
    n_l1 = push(rows_of(O1), rows_of(R1), left)
    n_mid = push(halo_of(O1), halo_of(R1), left)
    tails = [push(tail, halo_of(L0), dev(jnp.where(x == 3, sp_next, sp), xat(2)))]
    edges = [remote(tail, edge, dev(sp_next, xat(j))) for j in (0, 1, 3)]
    edge_from = {0: 3, 1: 0, 3: 2}

    @pl.when(x == 3)
    def _():
        for cp in edges:
            cp.start()

    n_r1 = push(rows_of(O1), rows_of(L1), right)
    n_l0 = push(rows_of(O0), rows_of(R0), left)

    phase("u3a")
    g_u.s3((0,))
    phase("u3b")
    g_u.s3((-1,))
    phase("u3c")
    g_u.s3((1,))
    g_d.s1q(0)
    phase("u3d")
    g_u.s3((2,))
    g_d.s1q(-1)
    g_d.s1q(1)
    phase("d2")
    g_d.s2()
    phase("u4a")
    g_u.s4((0, -1))
    phase("n_half")
    n_r0.wait_recv()
    f_r = push(rows_of(L0), rows_of(A0), right)
    n_l1.wait_recv()
    f_l = push(rows_of(R1), rows_of(A1), left)
    phase("u4c")
    g_u.s4((1, 2))
    phase("d3a")
    g_d.s3((0,))
    phase("u5")
    g_u.s5()
    phase("tails")
    n_mid.wait_recv()
    for cp in tails:
        cp.wait_recv()
    for j, cp in zip((0, 1, 3), edges):

        @pl.when(x == edge_from[j])
        def _(cp=cp):
            cp.wait_recv()

    def put_halo(slot, before, edge_x):
        near = nb[before, HALF:EXT, :]
        nb[slot, 0:HALO, :] = jnp.where(x == edge_x, edge[...], near)

    def up(i, to, parts=(0, 1)):
        rows = nb[i : i + 2].reshape(PAIR, D)
        for h in parts:
            col = pl.ds(h * HID, HID)
            to[:, col] = ceil_dot(rows, wu[:, col]).astype(BF16).astype(F32)

    def conv(i, pre, blocks):
        def step(j, _):
            gc = pl.ds(pl.multiple_of(j * 128, 128), 128)
            vc = pl.ds(pl.multiple_of(HID + j * 128, 128), 128)
            tg = cg[:, gc]
            tv = cv[:, gc]
            for n, (d, h) in enumerate(blocks):
                for r in range(0, HALF, 64):
                    mr = pl.ds(pl.multiple_of(d * BLK + h * HALF + r, 64), 64)
                    k1 = m1[mr, :] > 0.5
                    k2 = m2[mr, :] > 0.5
                    r0 = n * EXT + HALO + r

                    def taps(t, cc):
                        a = t[2:3] * pre[r0 : r0 + 64, cc]
                        a = a + jnp.where(k1, t[1:2] * pre[r0 - 1 : r0 + 63, cc], 0.0)
                        return a + jnp.where(k2, t[0:1] * pre[r0 - 2 : r0 + 62, cc], 0.0)

                    g = taps(tg, gc)
                    v = taps(tv, vc)
                    o = n * HALF + r
                    hid[i // 2, o : o + 64, gc] = (g / (1.0 + jnp.exp(-g)) * v).astype(BF16)
            return 0

        lax.fori_loop(0, HID // 128, step, 0)

    chunks = (pl.ds(0, 1024), pl.ds(1024, 1024))
    top, bot = pl.ds(0, HALF), pl.ds(HALF, HALF)

    def down(i, col):
        return nt_dot(hid[i // 2], wd[col, :])

    phase("up1")
    up(R1, pre)
    phase("d3b")
    g_d.s3((-1, 1))
    phase("d3c")
    g_d.s3((2,))
    g_d.s4((0,))
    phase("conv1")
    conv(R1, pre, ((xat(1), 1), (xat(3), 0)))
    phase("d4a")
    g_d.s4((-1, 1))
    phase("d4b")
    g_d.s4((2,))
    phase("d5")
    g_d.s5()
    phase("down1")
    s_one, s_two, s_three = [], [], []
    for col in chunks:
        a = down(R1, col)
        s1[:, col] = a.astype(BF16)
        s_one.append(push(s1.at[top, col], rl.at[bot, col], right))
        s_one.append(push(s1.at[bot, col], rr.at[top, col], left))

    n_r1.wait_recv()
    put_halo(O0, L1, 0)
    phase("up0a")
    up(O0, pre0, (0,))

    phase("wait_n2")
    f_r.wait_recv()
    f_l.wait_recv()
    nb[A1, 0:HALO, :] = nb[A0, HALF:EXT, :]
    put_halo(A0, R1, 2)
    phase("up2")
    up(A0, pre)
    phase("conv2")
    conv(A0, pre, ((xat(2), 0), (xat(2), 1)))
    phase("down2")
    for col in chunks:
        s2[:, col] = down(A0, col).astype(BF16)
        s_two.append(
            (
                push(s2.at[top, col], tl.at[:, col], right),
                push(s2.at[bot, col], tr.at[:, col], left),
            )
        )

    phase("wait_n1")
    n_l0.wait_recv()
    nb[L1, 0:HALO, :] = nb[L0, HALF:EXT, :]
    put_halo(R0, O1, 3)
    phase("up3")
    up(R0, pre)
    phase("conv3")
    conv(R0, pre, ((xat(1), 0), (xat(3), 1)))
    phase("down3")
    for col in chunks:
        p3[:, col] = down(R0, col)

    def finish(i, col):
        s_two[i][0].wait_recv()
        s3[top, col] = (p3[top, col] + tl[:, col].astype(F32)).astype(BF16)
        s_three.append(push(s3.at[top, col], rl.at[top, col], right))
        s_two[i][1].wait_recv()
        s3[bot, col] = (p3[bot, col] + tr[:, col].astype(F32)).astype(BF16)
        s_three.append(push(s3.at[bot, col], rr.at[bot, col], left))

    phase("wait_t0")
    finish(0, chunks[0])

    phase("up0b")
    up(O0, pre0, (1,))
    phase("conv0")
    conv(O0, pre0, ((x, 0), (x, 1)))
    phase("wait_t1")
    finish(1, chunks[1])
    phase("down0")
    for col in chunks:
        mid[:, col] += down(O0, col)

    phase("wait_s1")
    for cp in s_one:
        cp.wait_recv()
    for i, col in enumerate(chunks):
        phase("wait_s3")
        s_three[2 * i].wait_recv()
        s_three[2 * i + 1].wait_recv()
        phase("final")
        out[:, col] = (mid[:, col] + rl[:, col].astype(F32) + rr[:, col].astype(F32)).astype(BF16)
    phase("wait_sends")
    for cp in copies:
        cp.wait_send()

    @pl.when(x == 3)
    def _():
        for cp in edges:
            cp.wait_send()

    @pl.when(jnp.logical_not(last))
    def _():
        h_kv.wait_send()
        h_drow.wait_send()

    for g in (g_o, g_u, g_d):
        g.gone()
    phase(None)
    assert used["s"] <= N_SEND and used["r"] <= N_RECV, used


def per_device(
    queries,
    keys,
    values,
    doc_ids,
    sinks,
    residual,
    out_weight,
    norm_gain,
    w_gate,
    w_value,
    conv_gate,
    conv_value,
    w_down,
):
    drow = doc_ids.reshape(8, 128)
    wdt = w_down.T
    any_spec = pl.BlockSpec(memory_space=pl.ANY)
    smem = pl.BlockSpec(memory_space=pltpu.SMEM)
    V = pltpu.VMEM
    i32 = jnp.int32
    return pl.pallas_call(
        kernel,
        out_shape=pltpu.VMEM((BLK, D), BF16),
        in_specs=[any_spec] * 4 + [smem] + [any_spec] * 8,
        out_specs=pl.BlockSpec(memory_space=pltpu.VMEM),
        scratch_shapes=[
            V((ROWS, 256), BF16),
            V((128, ROWS + WINDOW), BF16),
            V((ROWS + WINDOW, 2048), BF16),
            V((16, 128), i32),
            V((ROWS + HALO, 128), F32),
            V((ROWS, 128), F32),
            V((ROWS, 128), F32),
            V((ROWS, 256), BF16),
            V((BLK, 1024), BF16),
            V((2, HALF, 256), BF16),
            V((4, 256, D), BF16),
            V((BLK, D), BF16),
            V((BLK, D), F32),
            V((1, D), F32),
            V((8, EXT, D), BF16),
            V((HALO, D), BF16),
            V((D, 2 * HID), BF16),
            V((D, HID), BF16),
            V((PAIR, 2 * HID), F32),
            V((PAIR, 2 * HID), F32),
            V((4, BLK, HID), BF16),
            V((3, HID), F32),
            V((3, HID), F32),
            V((BLK, D), BF16),
            V((BLK, D), BF16),
            V((BLK, D), BF16),
            V((BLK, D), F32),
            V((BLK, D), BF16),
            V((BLK, D), BF16),
            V((128, D), BF16),
            V((128, D), BF16),
            pltpu.SemaphoreType.DMA((N_SEND,)),
            pltpu.SemaphoreType.DMA((N_RECV,)),
            pltpu.SemaphoreType.DMA((16,)),
        ],
        compiler_params=pltpu.CompilerParams(
            collective_id=0,
            has_side_effects=True,
            vmem_limit_bytes=62_000_000,
        ),
        cost_estimate=pl.CostEstimate(
            flops=20_000_000_000, bytes_accessed=10_000_000, transcendentals=4_000_000
        ),
    )(
        queries,
        keys.T,
        values.T,
        drow,
        sinks,
        residual,
        out_weight,
        norm_gain.reshape(1, D),
        w_gate,
        w_value,
        conv_gate,
        conv_value,
        wdt,
    )


def solution(mesh):
    return jax.shard_map(
        per_device,
        mesh=mesh,
        in_specs=(
            P("sp", "tp"),
            P("sp", "tp"),
            P("sp", "tp"),
            P("sp"),
            P("tp"),
            P(("sp", "tp"), None),
            P("tp", None),
            P(),
            P("sp", "tp"),
            P("sp", "tp"),
            P(None, "tp"),
            P(None, "tp"),
            P("tp", "sp"),
        ),
        out_specs=P(("sp", "tp"), None),
        check_vma=False,
    )
```
